512 devices in a mesh: rep: 2 (over z_hi), fs: 32 (over z_lo, y), tp: 8 (over x, core).
Axes of the slice: x: 4, y: 8, z: 8 (z_hi: 2, z_lo: 4; z = z_hi * 4 + z_lo), core: 2. Of those that a mesh axis runs over, the one named last changes fastest.
Arguments:
- tokens: bfloat16 [8192, 2048], P(('rep', 'fs')), may hold values from -6 to 6
- attention_norm_gain: float32 [2048], replicated, may hold values from 0.1 to 1.9
- query_weight: bfloat16 [2048, 1024], P('fs', 'tp'), may hold values from -0.125 to 0.125
- key_weight: bfloat16 [2048, 1024], P('fs', 'tp'), may hold values from -0.125 to 0.125
- value_weight: bfloat16 [2048, 2048], P('fs', 'tp'), may hold values from -0.125 to 0.125
- decay_weight: bfloat16 [2048, 1024], P('fs', 'tp'), may hold values from -0.125 to 0.125
- decay_gate_bias: float32 [1024], P('tp'), may hold values from -1.5 to 5.5
- decay_spike_extra: float32 [8192, 32], P(('rep', 'fs'), 'tp'), may hold values from -0.7 to 0
- head_output_gain: float32 [64], replicated, may hold values from 0.1 to 1.9
- output_weight: bfloat16 [2048, 2048], P('fs', 'tp'), may hold values from -0.125 to 0.125
- channel_norm_gain: float32 [2048], replicated, may hold values from 0.1 to 1.9
- gate_weight: bfloat16 [2048, 3072], P('fs', 'tp'), may hold values from -0.125 to 0.125
- up_weight: bfloat16 [2048, 3072], P('fs', 'tp'), may hold values from -0.125 to 0.125
- down_weight: bfloat16 [2048, 3072], P('fs', 'tp'), may hold values from -0.109375 to 0.109375
Outputs:
- layer_out: bfloat16 [8192, 2048], P(('rep', 'fs'))
The draws below stay inside these ranges and needn't reach their ends.
All inputs are finite; a program needn't handle non-finite values.
Results may differ from the reference program's by a relative error of at most 0.018.
Values may be sent and summed in bfloat16 or wider, within the bound.
A program may use at most 64 MiB of HBM per device.

```python
import jax
import jax.numpy as jnp
from jax import lax

D = 2048
HEAD_K = 32
HEAD_V = 64
HEADS = 32
FF = 3072
BLOCK = 64
TOK_GROUP = 128
TOKENS = 8192
N_TP = 8


def draw_decay_gate_bias(key, part):
    keys_all = jax.random.split(key, 4)
    fast_share = 0.5
    is_fast = jax.random.uniform(keys_all[0], (HEADS,), jnp.float32) < fast_share
    fast_value = jax.random.uniform(keys_all[1], (HEADS,), jnp.float32, -1.0, 0.0)
    slow_value = jax.random.uniform(keys_all[2], (HEADS,), jnp.float32, 3.0, 5.0)
    base_value = jnp.where(is_fast, fast_value, slow_value)
    jitter = jax.random.uniform(keys_all[3], (HEADS, HEAD_K), jnp.float32, -0.5, 0.5)
    return (base_value[:, None] + jitter).reshape(HEADS * HEAD_K).astype(jnp.float32)


def draw_decay_spike_extra(key, part):
    keys_all = jax.random.split(key, 2)
    chosen = jax.random.uniform(keys_all[0], (TOKENS, HEADS), jnp.float32) < 3.0 / TOK_GROUP
    depth = jax.random.uniform(keys_all[1], (TOKENS, HEADS), jnp.float32, -0.7, -0.22)
    return jnp.where(chosen, depth, 0.0).astype(jnp.float32)


def levels(own_key, extent, cuts, smallest, high):
    loudness, own = 1.0, jax.random.fold_in(own_key, 6)
    for position, blocks in cuts:
        draws = jnp.exp(jax.random.uniform(jax.random.fold_in(own, position), (blocks,), jnp.float32, smallest / len(cuts), high / len(cuts)))
        loudness = loudness * jnp.repeat(draws, extent[position] // blocks).reshape([-1 if axis == position else 1 for axis in range(len(extent))])
    return loudness


def bell_draw(own_key, extent, deviation, bound, shards=(), kind=jnp.bfloat16):
    values = deviation * jax.random.normal(own_key, extent, jnp.float32)
    if shards:
        values = values * levels(own_key, extent, shards, -0.22, 0.18)
    return jnp.clip(values, -bound, bound).astype(kind)


def setup_inputs(seed: int = 0) -> dict:
    seeds = jax.random.split(jax.random.key(seed), 15)
    return {
        "tokens": bell_draw(seeds[0], (TOKENS, D), 1.0, 6.0, ((0, 64),)),
        "attention_norm_gain": jnp.clip(1.0 + 0.18 * jax.random.normal(seeds[1], (D,), jnp.float32), 0.1, 1.9),
        "query_weight": bell_draw(seeds[2], (D, HEADS * HEAD_K), D ** -0.5, 0.125, ((0, 32), (1, 8))),
        "key_weight": bell_draw(seeds[3], (D, HEADS * HEAD_K), D ** -0.5, 0.125, ((0, 32), (1, 8))),
        "value_weight": bell_draw(seeds[4], (D, HEADS * HEAD_V), D ** -0.5, 0.125, ((0, 32), (1, 8))),
        "decay_weight": bell_draw(seeds[5], (D, HEADS * HEAD_K), D ** -0.5, 0.125, ((0, 32), (1, 8))),
        "decay_gate_bias": draw_decay_gate_bias(jax.random.fold_in(seeds[14], 71), 0),
        "decay_spike_extra": draw_decay_spike_extra(jax.random.fold_in(seeds[14], 71), 0),
        "head_output_gain": jnp.clip(1.0 + 0.18 * jax.random.normal(seeds[8], (HEAD_V,), jnp.float32), 0.1, 1.9),
        "output_weight": bell_draw(seeds[9], (D, HEADS * HEAD_V), (HEADS * HEAD_V) ** -0.5, 0.125, ((0, 32), (1, 8))),
        "channel_norm_gain": jnp.clip(1.0 + 0.18 * jax.random.normal(seeds[10], (D,), jnp.float32), 0.1, 1.9),
        "gate_weight": bell_draw(seeds[11], (D, FF), D ** -0.5, 0.125, ((0, 32), (1, 8))),
        "up_weight": bell_draw(seeds[12], (D, FF), D ** -0.5, 0.125, ((0, 32), (1, 8))),
        "down_weight": bell_draw(seeds[13], (D, FF), FF ** -0.5, 0.109375, ((0, 32), (1, 8))),
    }


GATE_NORM = 16.0
NORM_EPS = 1e-06
HIGHEST = lax.Precision.HIGHEST

def rms_scale(values, scales):
    floats = values.astype(jnp.float32)
    return floats * lax.rsqrt(lax.optimization_barrier(jnp.mean(floats * floats, axis=-1, keepdims=True)) + NORM_EPS) * scales

def one_way(queries, key_rows, value_rows, decay_logarithm):
    length, number_of_heads, key_width = queries.shape
    value_width = value_rows.shape[2]
    block_count = length // BLOCK

    def blocks(tensor):
        return tensor.reshape(block_count, BLOCK, number_of_heads, tensor.shape[2]).transpose(0, 2, 1, 3)
    lower_mask = jnp.tril(jnp.ones((BLOCK, BLOCK), bool))

    def advance(carried, pieces):
        query_part, key_part, value_part, decay_part = pieces
        running = jnp.cumsum(decay_part, axis=1)
        spread = jnp.where(lower_mask[None, :, :, None], running[:, :, None, :] - running[:, None, :, :], -jnp.inf)
        scores = jnp.einsum('hid,hjd,hijd->hij', query_part, key_part, jnp.exp(spread), precision=HIGHEST)
        block_end = running[:, -1:, :]
        result = jnp.einsum('hij,hje->hie', scores, value_part, precision=HIGHEST)
        result = result + jnp.einsum('hid,hde->hie', query_part * jnp.exp(running), carried, precision=HIGHEST)
        carried = jnp.exp(block_end)[:, 0, :, None] * carried + jnp.einsum('hjd,hje->hde', key_part * jnp.exp(block_end - running), value_part, precision=HIGHEST)
        return (carried, result)
    zero_state = jnp.zeros((number_of_heads, key_width, value_width), jnp.float32)
    _, outputs = lax.scan(advance, zero_state, (blocks(queries), blocks(key_rows), blocks(value_rows), blocks(decay_logarithm)))
    return outputs.transpose(0, 2, 1, 3).reshape(length, number_of_heads, value_width)

def both_ways(queries, key_rows, value_rows, decay_logarithm):
    forward = one_way(queries, key_rows, value_rows, decay_logarithm)
    backward = one_way(jnp.flip(queries, 0), jnp.flip(key_rows, 0), jnp.flip(value_rows, 0), jnp.flip(decay_logarithm, 0))
    return forward + jnp.flip(backward, 0)

def rounded(floats):
    return lax.optimization_barrier(floats.astype(jnp.bfloat16)).astype(jnp.float32)

def grouped_sum(left, right):
    width = left.shape[1] // N_TP
    total = jnp.zeros((left.shape[0], right.shape[0]), jnp.float32)
    for shard_id in range(N_TP):
        part_left = left[:, shard_id * width:(shard_id + 1) * width]
        part_right = right[:, shard_id * width:(shard_id + 1) * width]
        partial_sum = lax.dot_general(part_left, part_right, (((1,), (1,)), ((), ())), preferred_element_type=jnp.float32)
        total = total + rounded(partial_sum)
    return total

def reference(tokens, attention_norm_gain, query_weight, key_weight, value_weight, decay_weight, decay_gate_bias, decay_spike_extra, head_output_gain, output_weight, channel_norm_gain, gate_weight, up_weight, down_weight):
    normed = rms_scale(tokens, attention_norm_gain).astype(jnp.bfloat16)
    queries = jnp.dot(normed, query_weight, preferred_element_type=jnp.float32).astype(jnp.bfloat16)
    key_rows = jnp.dot(normed, key_weight, preferred_element_type=jnp.float32).astype(jnp.bfloat16)
    value_rows = jnp.dot(normed, value_weight, preferred_element_type=jnp.float32).astype(jnp.bfloat16)
    gate_pre = jnp.dot(normed, decay_weight, preferred_element_type=jnp.float32)
    decay_logarithm = jax.nn.log_sigmoid(gate_pre + decay_gate_bias).reshape(TOKENS, HEADS, HEAD_K) / GATE_NORM
    decay_logarithm = decay_logarithm + decay_spike_extra[:, :, None]
    seq_count = TOKENS // TOK_GROUP
    query_seq = (queries.astype(jnp.float32) * HEAD_K ** (-0.5)).reshape(seq_count, TOK_GROUP, HEADS, HEAD_K)
    key_seq = key_rows.astype(jnp.float32).reshape(seq_count, TOK_GROUP, HEADS, HEAD_K)
    value_seq = value_rows.astype(jnp.float32).reshape(seq_count, TOK_GROUP, HEADS, HEAD_V)
    decay_seq = decay_logarithm.reshape(seq_count, TOK_GROUP, HEADS, HEAD_K)

    def attend(pieces):
        mixed_heads = both_ways(*pieces)
        normed_heads = rms_scale(mixed_heads, head_output_gain)
        return normed_heads.reshape(TOK_GROUP, HEADS * HEAD_V).astype(jnp.bfloat16)
    attended = lax.map(attend, (query_seq, key_seq, value_seq, decay_seq)).reshape(TOKENS, HEADS * HEAD_V)
    residual = (tokens.astype(jnp.float32) + grouped_sum(attended, output_weight)).astype(jnp.bfloat16)
    normed_two = rms_scale(residual, channel_norm_gain).astype(jnp.bfloat16)
    gate_pre_two = jnp.dot(normed_two, gate_weight, preferred_element_type=jnp.float32)
    up_proj = jnp.dot(normed_two, up_weight, preferred_element_type=jnp.float32)
    hidden = (jax.nn.silu(gate_pre_two) * up_proj).astype(jnp.bfloat16)
    return (residual.astype(jnp.float32) + grouped_sum(hidden, down_weight)).astype(jnp.bfloat16)
```

```python
import functools

import jax
import jax.numpy as jnp
from jax import lax
from jax.experimental import pallas as pl
from jax.experimental.pallas import tpu as pltpu
from jax.sharding import PartitionSpec as P

MESH = pl.DeviceIdType.MESH
F32, BF16 = jnp.float32, jnp.bfloat16
NY, NZ, NTP = 8, 4, 8
SEQ, D = 128, 2048
SLAB = D // (NY * NZ)
HEADS, KW, VW = 4, 32, 64
LEVELS = 7
EPS = 1e-6
PARTS = ((128, 128, 256, 128), (256,), (384, 384), (384,))
A_ROWS = (((0, 16), (16, 16)),) * 4
B_ROWS = (((32, 16), (48, 16)),) * 4
ROWS_OWN = SEQ // NTP


def dot(a, b):
    return jnp.dot(a, b, preferred_element_type=F32)


def dot_t(a, b):
    return lax.dot_general(a, b, (((1,), (1,)), ((), ())), preferred_element_type=F32)


def iota(shape, axis):
    return lax.broadcasted_iota(jnp.int32, shape, axis)


def layer_kernel(
    tok, gain1, bias, spike, hgain, gain2, wq, wk, wv, wd, wo, wg, wu, wdn,
    out,
    g1, g2, g3, g4, xn, acc, mats, score, att, part, got, n2, acc2, hid, part2, got2, resid, decay2, qf, kf, vbd,
    lsem, send, recv, tsend, trecv,
):
    bufs = (g1, g2, g3, g4)
    rep, f, t = lax.axis_index("rep"), lax.axis_index("fs"), lax.axis_index("tp")
    y, z = lax.rem(f, NY), lax.div(f, NY)
    zz = rep * NZ + z

    def at_y(k):
        return (rep, z * NY + lax.rem(y + k + NY, NY), t)

    def at_z(k):
        w = lax.rem(zz + k + 2 * NZ, 2 * NZ)
        return (lax.div(w, NZ), lax.rem(w, NZ) * NY + y, t)

    ynb, znb = (at_y(1), at_y(-1)), (at_z(1), at_z(-1))

    def peer(k):
        return (rep, f, lax.rem(t + k, NTP))

    own = []
    srcs = ((wq, wk, wv, wd), (wo,), (wg, wu), (wdn,))
    n = 0
    for g in range(4):
        at, copies = 0, []
        for src, width in zip(srcs[g], PARTS[g]):
            copies.append(pltpu.make_async_copy(src, bufs[g].at[z, y, :, at : at + width], lsem.at[n]))
            at += width
            n += 1
        for c in copies:
            c.start()
        own.append(copies)

    barrier = pltpu.get_barrier_semaphore()
    others = [*ynb, *znb, *(peer(k) for k in range(1, NTP))]
    for d in others:
        pl.semaphore_signal(barrier, inc=1, device_id=d, device_id_type=MESH)
    pl.semaphore_wait(barrier, len(others))

    base = (0, 16, 24, 32)

    def wrap_y(k):
        return lax.rem(y + k + NY, NY)

    def wrap_z(k):
        return lax.rem(z + k + NZ, NZ)

    def piece(g, kind, u, off):
        start, size = (A_ROWS if kind in (0, 2) else B_ROWS)[g][u]
        rows = slice(start, start + size)
        b = bufs[g]
        if kind == 0:
            return b.at[z, wrap_y(off), rows, :]
        if kind == 3:
            return b.at[:, wrap_y(off), rows, :]
        if kind == 1:
            return b.at[wrap_z(off), y, rows, :]
        return b.at[wrap_z(off), :, rows, :]

    def sem_of(kind, s, d, u):
        per = 8 if kind in (0, 3) else 4
        return base[kind] + d * per + s * 2 + u

    def message(g, kind, s, d, u, arriving):
        sign = -1 if d == 0 else 1
        ref = piece(g, kind, u, sign * (s + 1 if arriving else s))
        i = sem_of(kind, s, d, u)
        return pltpu.make_async_remote_copy(
            src_ref=ref,
            dst_ref=ref,
            send_sem=send.at[g, i],
            recv_sem=recv.at[g, i],
            device_id=(ynb if kind in (0, 3) else znb)[d],
            device_id_type=MESH,
        )

    started = []

    def start(g, kind, s, d, u):
        m = message(g, kind, s, d, u, False)
        m.start()
        started.append(m)

    def arrive(g, kind, s, d, u):
        message(g, kind, s, d, u, True).wait_recv()

    def last(kind):
        return 3 if kind in (0, 3) else 1

    def begin(g, kind):
        for u in (0, 1):
            for d in (0, 1):
                start(g, kind, 0, d, u)

    def step(g, kind, s):
        for u in (0, 1):
            for d in (0, 1):
                arrive(g, kind, s - 1, d, u)
                if s < last(kind) or u == d:
                    start(g, kind, s, d, u)

    def finish(g, kind):
        for d in (0, 1):
            arrive(g, kind, last(kind), d, d)

    def comm():
        def light(g):
            for c in own[g]:
                c.wait()
            begin(g, 0)
            begin(g, 1)
            yield
            step(g, 0, 1)
            step(g, 1, 1)
            yield
            step(g, 0, 2)
            yield
            step(g, 0, 3)
            finish(g, 1)
            yield
            finish(g, 0)

        def heavy(g):
            begin(g, 3)
            begin(g, 2)
            yield
            step(g, 3, 1)
            yield
            step(g, 3, 2)
            yield
            step(g, 2, 1)
            step(g, 3, 3)
            yield
            finish(g, 2)
            finish(g, 3)

        yield from light(0)
        for g in range(4):
            a, b = heavy(g), light(g + 1) if g < 3 else iter(())
            more = True
            while more:
                more = False
                for it in (a, b):
                    if next(it, "end") is None:
                        more = True
                        yield
            yield g

    stream = comm()
    done = [-1]

    def pump(n=1):
        for _ in range(n):
            r = next(stream, None)
            if r is not None:
                done[0] = r

    def until(g):
        while done[0] < g:
            pump()

    pump()

    def norm_rows(i, c):
        r = pl.ds(pl.multiple_of(i * 16, 16), 16)
        v = tok[r, :].astype(F32)
        xn[r, :] = (v * lax.rsqrt(jnp.mean(v * v, axis=-1, keepdims=True) + EPS) * gain1[...]).astype(BF16)
        return c

    lax.fori_loop(0, SEQ // 16, norm_rows, 0)
    pump()

    def build_mats(l, c):
        ti, si = iota((SEQ, 2 * SEQ), 0), lax.rem(iota((SEQ, 2 * SEQ), 1), SEQ)
        same = lax.shift_right_logical(ti, l) == lax.shift_right_logical(si, l)
        back = (ti - si) * (2 * (lax.shift_right_logical(ti, l) & 1) - 1)
        mats[2 * l] = jnp.where(same & (back >= 0), 1.0, 0.0).astype(BF16)
        mats[2 * l + 1] = jnp.where(same & (back > 0), 1.0, 0.0).astype(BF16)
        return c

    lax.fori_loop(0, LEVELS, build_mats, 0)
    until(0)
    pump(2)

    acc[...] = jnp.zeros_like(acc)

    def project(w, c):
        cols = pl.ds(pl.multiple_of(w * 512, 512), 512)
        acc[...] += dot(xn[:, cols], g1[w].reshape(512, 640))
        return c

    lax.fori_loop(0, NZ, project, 0)
    pump()
    gate = acc[:, 512:640] + bias[...]
    lane_head = lax.div(iota((SEQ, 128), 1), KW)
    extra = jnp.zeros((SEQ, 128), F32)
    for h in range(HEADS):
        extra = jnp.where(lane_head == h, spike[:, h : h + 1], extra)
    logs = (jnp.minimum(gate, 0.0) - jnp.log1p(jnp.exp(-jnp.abs(gate)))) / 16.0 + extra
    hi = logs.astype(BF16)
    decay2[0:SEQ, :] = hi
    decay2[SEQ : 2 * SEQ, :] = (logs - hi.astype(F32)).astype(BF16)
    qf[...] = acc[:, 0:128].astype(BF16).astype(F32)
    kf[...] = acc[:, 128:256].astype(BF16).astype(F32)
    vals = acc[:, 256:512]
    lane_vhead = lax.div(iota((SEQ, 256), 1), VW)
    for h in range(HEADS):
        vbd[h * SEQ : (h + 1) * SEQ, :] = jnp.where(lane_vhead == h, vals, 0.0).astype(BF16)

    def by_head(x):
        return jnp.concatenate([jnp.where(lane_head == h, x, 0.0).astype(BF16) for h in range(HEADS)], axis=0)

    score[...] = 2.0 * dot_t(qf[...].astype(BF16), by_head(kf[...]))
    pump()

    def level(l, c):
        left = (qf[...] * jnp.exp(dot(mats[2 * l], decay2[...]))).astype(BF16)
        right = by_head(kf[...] * jnp.exp(dot(mats[2 * l + 1], decay2[...])))
        differ = iota((SEQ, HEADS * SEQ), 0) ^ lax.rem(iota((SEQ, HEADS * SEQ), 1), SEQ)
        score[...] = jnp.where(differ >= lax.shift_left(1, l), dot_t(left, right), score[...])
        return c

    for lo, hi_ in ((0, 2), (2, 4), (4, 6), (6, 7)):
        lax.fori_loop(lo, hi_, level, 0)
        pump()
    mixed = dot(score[...].astype(BF16), vbd[...]) * (KW ** -0.5)
    sq = mixed * mixed
    sq_hi = sq.astype(BF16)
    sq_lo = (sq - sq_hi.astype(F32)).astype(BF16)
    ones = jnp.where(lax.div(iota((256, 256), 0), VW) == lax.div(iota((256, 256), 1), VW), 1.0, 0.0).astype(BF16)
    mean = (dot(sq_hi, ones) + dot(sq_lo, ones)) * (1.0 / VW)
    att[...] = (mixed * lax.rsqrt(mean + EPS) * hgain[...]).astype(BF16)
    until(1)
    pump(2)

    def project_out(left, weight, width, into):
        def body(w, c):
            cols = pl.ds(pl.multiple_of(w * 512, 512), 512)
            into[:, cols] = dot_t(left[...], weight[w].reshape(512, width)).astype(BF16)
            return c

        lax.fori_loop(0, NZ, body, 0)

    own_rows = pl.ds(pl.multiple_of(t * ROWS_OWN, ROWS_OWN), ROWS_OWN)

    def exchange(n, k, src, dst):
        return pltpu.make_async_remote_copy(
            src_ref=src, dst_ref=dst, send_sem=tsend.at[n, k], recv_sem=trecv.at[n, k],
            device_id=peer(k), device_id_type=MESH,
        )

    def scatter(n, src, dst):
        out_ = []
        for k in range(1, NTP):
            rows = pl.ds(pl.multiple_of(lax.rem(t + k, NTP) * ROWS_OWN, ROWS_OWN), ROWS_OWN)
            m = exchange(n, k, src.at[rows, :], dst.at[k])
            m.start()
            started.append(m)
            out_.append(m)
        return out_

    def spread(n, ref):
        for k in range(1, NTP):
            m = exchange(n, k, ref.at[own_rows, :], ref.at[own_rows, :])
            m.start()
            started.append(m)

    def spread_wait(n, ref):
        for k in range(1, NTP):
            rows = pl.ds(pl.multiple_of(lax.rem(t - k + NTP, NTP) * ROWS_OWN, ROWS_OWN), ROWS_OWN)
            exchange(n, k, ref.at[rows, :], ref.at[rows, :]).wait_recv()

    def total(src, dst):
        s = src[own_rows, :].astype(F32)
        for k in range(1, NTP):
            s = s + dst[k].astype(F32)
        return s

    project_out(att, g2, 256, part)
    moves = scatter(0, part, got)
    pump(2)
    for m in moves:
        m.wait_recv()
    residual = (tok[own_rows, :].astype(F32) + total(part, got)).astype(BF16).astype(F32)
    resid[...] = residual
    n2[own_rows, :] = (
        residual * lax.rsqrt(jnp.mean(residual * residual, axis=-1, keepdims=True) + EPS) * gain2[...]
    ).astype(BF16)
    spread(1, n2)
    pump(2)
    spread_wait(1, n2)
    until(2)
    pump(2)

    acc2[...] = jnp.zeros_like(acc2)

    def project2(w, c):
        cols = pl.ds(pl.multiple_of(w * 512, 512), 512)
        acc2[...] += dot(n2[:, cols], g3[w].reshape(512, 768))
        return c

    lax.fori_loop(0, NZ, project2, 0)
    pump()
    gated = acc2[:, 0:384]
    hid[...] = (gated / (1.0 + jnp.exp(-gated)) * acc2[:, 384:768]).astype(BF16)
    until(3)
    project_out(hid, g4, 384, part2)
    for m in scatter(2, part2, got2):
        m.wait_recv()
    out[own_rows, :] = (resid[...] + total(part2, got2)).astype(BF16)
    spread(3, out)
    spread_wait(3, out)
    for m in started:
        m.wait_send()


def shards(
    tokens, attention_norm_gain, query_weight, key_weight, value_weight, decay_weight, decay_gate_bias,
    decay_spike_extra, head_output_gain, output_weight, channel_norm_gain, gate_weight, up_weight, down_weight,
):
    vmem = pl.BlockSpec(memory_space=pltpu.VMEM)
    hbm = pl.BlockSpec(memory_space=pl.ANY)
    widths = [sum(p) for p in PARTS]
    return pl.pallas_call(
        layer_kernel,
        out_shape=jax.ShapeDtypeStruct((SEQ, D), BF16),
        in_specs=[vmem] * 6 + [hbm] * 8,
        out_specs=vmem,
        scratch_shapes=[
            *(pltpu.VMEM((NZ, NY, SLAB, w), BF16) for w in widths),
            pltpu.VMEM((SEQ, D), BF16),
            pltpu.VMEM((SEQ, 640), F32),
            pltpu.VMEM((2 * LEVELS, SEQ, 2 * SEQ), BF16),
            pltpu.VMEM((SEQ, HEADS * SEQ), F32),
            pltpu.VMEM((SEQ, 256), BF16),
            pltpu.VMEM((SEQ, D), BF16),
            pltpu.VMEM((NTP, ROWS_OWN, D), BF16),
            pltpu.VMEM((SEQ, D), BF16),
            pltpu.VMEM((SEQ, 768), F32),
            pltpu.VMEM((SEQ, 384), BF16),
            pltpu.VMEM((SEQ, D), BF16),
            pltpu.VMEM((NTP, ROWS_OWN, D), BF16),
            pltpu.VMEM((ROWS_OWN, D), F32),
            pltpu.VMEM((2 * SEQ, 128), BF16),
            pltpu.VMEM((SEQ, 128), F32),
            pltpu.VMEM((SEQ, 128), F32),
            pltpu.VMEM((HEADS * SEQ, 256), BF16),
            pltpu.SemaphoreType.DMA((8,)),
            pltpu.SemaphoreType.DMA((4, 48)),
            pltpu.SemaphoreType.DMA((4, 48)),
            pltpu.SemaphoreType.DMA((4, NTP)),
            pltpu.SemaphoreType.DMA((4, NTP)),
        ],
        compiler_params=pltpu.CompilerParams(collective_id=0, has_side_effects=True),
    )(
        tokens,
        attention_norm_gain.reshape(1, D),
        decay_gate_bias.reshape(1, 128),
        decay_spike_extra,
        jnp.tile(head_output_gain, HEADS).reshape(1, HEADS * VW),
        channel_norm_gain.reshape(1, D),
        query_weight, key_weight, value_weight, decay_weight, output_weight, gate_weight, up_weight, down_weight,
    )


def solution(mesh):
    rows, w = P(("rep", "fs"), None), P("fs", "tp")
    in_specs = (rows, P(), w, w, w, w, P("tp"), P(("rep", "fs"), "tp"), P(), w, P(), w, w, w)
    return jax.shard_map(shards, mesh=mesh, in_specs=in_specs, out_specs=rows, check_vma=False)
```

```python
import functools

import jax
import jax.numpy as jnp
from jax import lax
from jax.experimental import pallas as pl
from jax.experimental.pallas import tpu as pltpu
from jax.sharding import PartitionSpec as P

MESH = pl.DeviceIdType.MESH
F32, BF16 = jnp.float32, jnp.bfloat16
NY, NZ, NTP = 8, 4, 8
SEQ, D = 128, 2048
SLAB = D // (NY * NZ)
HEADS, KW, VW = 4, 32, 64
LEVELS = 7
EPS = 1e-6
PARTS = ((128, 128, 256, 128), (256,), (384, 384), (384,))
A_ROWS = (((0, 16), (16, 16)),) * 4
B_ROWS = (((32, 16), (48, 16)),) * 4
ROWS_OWN = SEQ // NTP


def link_plan(near, ahead, hop=2.6, rate=46.6e3, turn=6.5):
    units = (1, 1, 8, 4)
    cols = [sum(p) for p in PARTS]
    last = (3, 1, 1, 3)

    def rows(g, k, u):
        return (A_ROWS if k in (0, 2) else B_ROWS)[g][u][1]

    size = {
        (g, k, s, d, u): cols[g] * 2 * rows(g, k, u) * units[k]
        for g in range(4) for k in range(4) for s in range(last[k] + 1) for d in (0, 1) for u in (0, 1)
        if s < last[k] or u == d
    }

    def needs(m):
        g, k, s, d, u = m
        if s > 0:
            return {(g, k, s - 1, d, u)}
        if k < 2:
            return set()
        return {x for x in size if x[0] == g and x[1] == k - 2 and x[4] == u} if k == 2 else {
            x for x in size if x[0] == g and x[1] == 1 and x[4] == u
        }

    need = {m: needs(m) for m in size}
    then = {}
    for m, xs in need.items():
        for x in xs:
            then.setdefault(x, []).append(m)

    def urgency(m):
        g, k, s, d, u = m
        return (g * 10 - (ahead if k < 2 else 0), s, u, d)

    def link(m):
        return (m[1] in (0, 3), m[3])

    ready = {(a, d): [] for a in (True, False) for d in (0, 1)}
    free = dict.fromkeys(ready, 0.0)
    left = [sum(m[0] == g for m in size) for g in range(4)]
    for m in size:
        if not need[m]:
            ready[link(m)].append(m)
    now, ops, have, coming, at = 0.2, [], set(), [], 0
    while at < len(WORK) or coming:
        for l, queue in ready.items():
            while queue and free[l] - now < near:
                m = min(queue, key=urgency)
                queue.remove(m)
                free[l] = max(now, free[l]) + size[m] / rate
                coming.append((free[l] + hop, len(ops), m))
                ops.append(("send", m))
                now += 0.02
        coming.sort()
        if coming and coming[0][0] <= now:
            m = coming.pop(0)[2]
            ops.append(("take", m))
            now += 0.02
            if isinstance(m, str):
                have.add(m)
                continue
            left[m[0]] -= 1
            if left[m[0]] == 0:
                have.add(m[0])
            for x in then.get(m, ()):
                need[x].discard(m)
                if not need[x]:
                    ready[link(x)].append(x)
        elif at < len(WORK) and all(q in have for q in WORK[at][2]):
            name, span, _, gives = WORK[at]
            at += 1
            now += span
            ops.append(("work", name))
            if gives:
                coming.append((now + turn, len(ops), gives))
        else:
            now = max(now, min(coming)[0])
    return ops


WORK = (
    ("norm", 0.92, (), None),
    ("mats", 0.42, (), None),
    ("project", 1.1, (0,), None),
    ("prepare", 0.8, (), None),
    *((f"level{l}", 0.34, (), None) for l in range(LEVELS)),
    ("attend", 0.5, (), None),
    ("mix_out", 0.9, (1,), "scatter1"),
    ("residual", 0.3, ("scatter1",), "spread1"),
    ("gate_up", 1.1, ("spread1", 2), None),
    ("hidden", 0.2, (), None),
    ("down", 1.1, (3,), "scatter2"),
    ("layer_out", 0.3, ("scatter2",), "spread2"),
    ("end", 0.1, ("spread2",), None),
)
NEAR, AHEAD = 1.0, 12


def dot(a, b):
    return jnp.dot(a, b, preferred_element_type=F32)


def dot_t(a, b):
    return lax.dot_general(a, b, (((1,), (1,)), ((), ())), preferred_element_type=F32)


def iota(shape, axis):
    return lax.broadcasted_iota(jnp.int32, shape, axis)


def layer_kernel(
    tok_hbm, gain1, bias, spike, hgain, gain2, wq, wk, wv, wd, wo, wg, wu, wdn,
    out,
    tok, extra, fin,
    g1, g2, g3, g4, xn, acc, mats, score, att, part, got, n2, acc2, hid, part2, got2, resid, decay2, qf, kf, vbd,
    lsem, send, recv, tsend, trecv,
):
    bufs = (g1, g2, g3, g4)
    rep, f, t = lax.axis_index("rep"), lax.axis_index("fs"), lax.axis_index("tp")
    y, z = lax.rem(f, NY), lax.div(f, NY)
    zz = rep * NZ + z

    def at_y(k):
        return (rep, z * NY + lax.rem(y + k + NY, NY), t)

    def at_z(k):
        w = lax.rem(zz + k + 2 * NZ, 2 * NZ)
        return (lax.div(w, NZ), lax.rem(w, NZ) * NY + y, t)

    ynb, znb = (at_y(1), at_y(-1)), (at_z(1), at_z(-1))

    def peer(k):
        return (rep, f, lax.rem(t + k, NTP))

    barrier = pltpu.get_barrier_semaphore()
    others = [*ynb, *znb, *(peer(k) for k in range(1, NTP))]
    for d in others:
        pl.semaphore_signal(barrier, inc=1, device_id=d, device_id_type=MESH)

    own = []
    srcs = ((wq, wk, wv, wd), (wo,), (wg, wu), (wdn,))
    n = 0
    for g in range(4):
        at, copies = 0, []
        for src, width in zip(srcs[g], PARTS[g]):
            copies.append(pltpu.make_async_copy(src, bufs[g].at[z, y, :, at : at + width], lsem.at[n]))
            at += width
            n += 1
        for c in copies:
            c.start()
        own.append(copies)
        if g == 0:
            tok_copy = pltpu.make_async_copy(tok_hbm, tok, lsem.at[8])
            tok_copy.start()

    pl.semaphore_wait(barrier, len(others))

    base = (0, 16, 24, 32)

    def wrap_y(k):
        return lax.rem(y + k + NY, NY)

    def wrap_z(k):
        return lax.rem(z + k + NZ, NZ)

    def piece(g, kind, u, off):
        start, size = (A_ROWS if kind in (0, 2) else B_ROWS)[g][u]
        rows = slice(start, start + size)
        b = bufs[g]
        if kind == 0:
            return b.at[z, wrap_y(off), rows, :]
        if kind == 3:
            return b.at[:, wrap_y(off), rows, :]
        if kind == 1:
            return b.at[wrap_z(off), y, rows, :]
        return b.at[wrap_z(off), :, rows, :]

    def sem_of(kind, s, d, u):
        per = 8 if kind in (0, 3) else 4
        return base[kind] + d * per + s * 2 + u

    def message(g, kind, s, d, u, arriving):
        sign = -1 if d == 0 else 1
        ref = piece(g, kind, u, sign * (s + 1 if arriving else s))
        i = sem_of(kind, s, d, u)
        return pltpu.make_async_remote_copy(
            src_ref=ref,
            dst_ref=ref,
            send_sem=send.at[g, i],
            recv_sem=recv.at[g, i],
            device_id=(ynb if kind in (0, 3) else znb)[d],
            device_id_type=MESH,
        )

    started = []

    def start(g, kind, s, d, u):
        m = message(g, kind, s, d, u, False)
        m.start()
        started.append(m)

    def arrive(g, kind, s, d, u):
        message(g, kind, s, d, u, True).wait_recv()

    def norm_rows(i, c):
        r = pl.ds(pl.multiple_of(i * 16, 16), 16)
        v = tok[r, :].astype(F32)
        xn[r, :] = (v * lax.rsqrt(jnp.mean(v * v, axis=-1, keepdims=True) + EPS) * gain1[...]).astype(BF16)
        return c

    def norm():
        tok_copy.wait()
        lax.fori_loop(0, SEQ // 16, norm_rows, 0)

    def build_mats(l, c):
        ti, si = iota((SEQ, 2 * SEQ), 0), lax.rem(iota((SEQ, 2 * SEQ), 1), SEQ)
        same = lax.shift_right_logical(ti, l) == lax.shift_right_logical(si, l)
        back = (ti - si) * (2 * (lax.shift_right_logical(ti, l) & 1) - 1)
        mats[2 * l] = jnp.where(same & (back >= 0), 1.0, 0.0).astype(BF16)
        mats[2 * l + 1] = jnp.where(same & (back > 0), 1.0, 0.0).astype(BF16)
        return c

    def build():
        lax.fori_loop(0, LEVELS, build_mats, 0)
        heads = jnp.where(lax.div(iota((HEADS, 128), 1), KW) == iota((HEADS, 128), 0), 1.0, 0.0)
        extra[...] = lax.dot_general(
            spike[...], heads, (((0,), (0,)), ((), ())), precision=lax.Precision.HIGHEST, preferred_element_type=F32
        )

    def project():
        acc[...] = jnp.zeros_like(acc)

        def body(w, c):
            cols = pl.ds(pl.multiple_of(w * 512, 512), 512)
            acc[...] += dot(xn[:, cols], g1[w].reshape(512, 640))
            return c

        lax.fori_loop(0, NZ, body, 0)

    lane_head = lax.div(iota((SEQ, 128), 1), KW)

    def by_head(x):
        return jnp.concatenate([jnp.where(lane_head == h, x, 0.0).astype(BF16) for h in range(HEADS)], axis=0)

    def prepare():
        gate = acc[:, 512:640] + bias[...]
        logs = (jnp.minimum(gate, 0.0) - jnp.log1p(jnp.exp(-jnp.abs(gate)))) / 16.0 + extra[...]
        hi = logs.astype(BF16)
        decay2[0:SEQ, :] = hi
        decay2[SEQ : 2 * SEQ, :] = (logs - hi.astype(F32)).astype(BF16)
        qf[...] = acc[:, 0:128].astype(BF16).astype(F32)
        kf[...] = acc[:, 128:256].astype(BF16).astype(F32)
        vals = acc[:, 256:512]
        lane_vhead = lax.div(iota((SEQ, 256), 1), VW)
        for h in range(HEADS):
            vbd[h * SEQ : (h + 1) * SEQ, :] = jnp.where(lane_vhead == h, vals, 0.0).astype(BF16)
        score[...] = 2.0 * dot_t(qf[...].astype(BF16), by_head(kf[...]))

    def level(l):
        left = (qf[...] * jnp.exp(dot(mats[2 * l], decay2[...]))).astype(BF16)
        right = by_head(kf[...] * jnp.exp(dot(mats[2 * l + 1], decay2[...])))
        differ = iota((SEQ, HEADS * SEQ), 0) ^ lax.rem(iota((SEQ, HEADS * SEQ), 1), SEQ)
        score[...] = jnp.where(differ >= 2 ** l, dot_t(left, right), score[...])

    def attend():
        mixed = dot(score[...].astype(BF16), vbd[...]) * (KW ** -0.5)
        sq = mixed * mixed
        sq_hi = sq.astype(BF16)
        sq_lo = (sq - sq_hi.astype(F32)).astype(BF16)
        ones = jnp.where(lax.div(iota((256, 256), 0), VW) == lax.div(iota((256, 256), 1), VW), 1.0, 0.0).astype(BF16)
        mean = (dot(sq_hi, ones) + dot(sq_lo, ones)) * (1.0 / VW)
        gains = jnp.concatenate([hgain[...]] * HEADS, axis=1)
        att[...] = (mixed * lax.rsqrt(mean + EPS) * gains).astype(BF16)

    def project_out(left, weight, width, into):
        def body(w, c):
            cols = pl.ds(pl.multiple_of(w * 512, 512), 512)
            into[:, cols] = dot_t(left[...], weight[w].reshape(512, width)).astype(BF16)
            return c

        lax.fori_loop(0, NZ, body, 0)

    def rows_of(k):
        return pl.ds(pl.multiple_of(lax.rem(t + k + NTP, NTP) * ROWS_OWN, ROWS_OWN), ROWS_OWN)

    own_rows = rows_of(0)

    def exchange(n, k, src, dst):
        return pltpu.make_async_remote_copy(
            src_ref=src, dst_ref=dst, send_sem=tsend.at[n, k], recv_sem=trecv.at[n, k],
            device_id=peer(k), device_id_type=MESH,
        )

    def go(copy):
        copy.start()
        started.append(copy)

    def scatter(n, src, dst):
        for k in range(1, NTP):
            go(exchange(n, k, src.at[rows_of(k), :], dst.at[k]))

    def scatter_wait(n, src, dst):
        for k in range(1, NTP):
            exchange(n, k, src.at[rows_of(k), :], dst.at[k]).wait_recv()

    def spread(n, src, ref):
        for k in range(1, NTP):
            go(exchange(n, k, src, ref.at[own_rows, :]))

    def spread_wait(n, src, ref):
        for k in range(1, NTP):
            exchange(n, k, src, ref.at[rows_of(-k), :]).wait_recv()

    def total(src, dst):
        s = src[own_rows, :].astype(F32)
        for k in range(1, NTP):
            s = s + dst[k].astype(F32)
        return s

    def mix_out():
        project_out(att, g2, 256, part)
        scatter(0, part, got)

    def residual_rows():
        r = (tok[own_rows, :].astype(F32) + total(part, got)).astype(BF16).astype(F32)
        resid[...] = r
        n2[own_rows, :] = (r * lax.rsqrt(jnp.mean(r * r, axis=-1, keepdims=True) + EPS) * gain2[...]).astype(BF16)
        spread(1, n2.at[own_rows, :], n2)

    def gate_up():
        acc2[...] = jnp.zeros_like(acc2)

        def body(w, c):
            cols = pl.ds(pl.multiple_of(w * 512, 512), 512)
            acc2[...] += dot(n2[:, cols], g3[w].reshape(512, 768))
            return c

        lax.fori_loop(0, NZ, body, 0)

    def hidden():
        gated = acc2[:, 0:384]
        hid[...] = (gated / (1.0 + jnp.exp(-gated)) * acc2[:, 384:768]).astype(BF16)

    def down():
        project_out(hid, g4, 384, part2)
        scatter(2, part2, got2)

    own_out = pltpu.make_async_copy(fin, out.at[own_rows, :], lsem.at[9])

    def layer_out():
        fin[...] = (resid[...] + total(part2, got2)).astype(BF16)
        spread(3, fin, out)
        own_out.start()

    def end():
        own_out.wait()

    work = dict(
        norm=norm, mats=build, project=project, prepare=prepare, attend=attend, mix_out=mix_out,
        residual=residual_rows, gate_up=gate_up, hidden=hidden, down=down, layer_out=layer_out, end=end,
        **{f"level{l}": functools.partial(level, l) for l in range(LEVELS)},
    )
    waits = dict(
        scatter1=lambda: scatter_wait(0, part, got), spread1=lambda: spread_wait(1, n2.at[own_rows, :], n2),
        scatter2=lambda: scatter_wait(2, part2, got2), spread2=lambda: spread_wait(3, fin, out),
    )
    waiting = set(range(4))
    for verb, what in link_plan(NEAR, AHEAD):
        with jax.named_scope(f"{verb}_{what}".replace(" ", "")):
            if verb == "work":
                work[what]()
            elif verb == "send":
                if what[0] in waiting:
                    waiting.discard(what[0])
                    for c in own[what[0]]:
                        c.wait()
                start(*what)
            elif isinstance(what, str):
                waits[what]()
            else:
                arrive(*what)
    for m in started:
        m.wait_send()


def shards(
    tokens, attention_norm_gain, query_weight, key_weight, value_weight, decay_weight, decay_gate_bias,
    decay_spike_extra, head_output_gain, output_weight, channel_norm_gain, gate_weight, up_weight, down_weight,
):
    vmem = pl.BlockSpec(memory_space=pltpu.VMEM)
    hbm = pl.BlockSpec(memory_space=pl.ANY)
    widths = [sum(p) for p in PARTS]
    return pl.pallas_call(
        layer_kernel,
        out_shape=jax.ShapeDtypeStruct((SEQ, D), BF16),
        in_specs=[hbm] + [vmem] * 5 + [hbm] * 8,
        out_specs=hbm,
        scratch_shapes=[
            pltpu.VMEM((SEQ, D), BF16),
            pltpu.VMEM((SEQ, 128), F32),
            pltpu.VMEM((ROWS_OWN, D), BF16),
            *(pltpu.VMEM((NZ, NY, SLAB, w), BF16) for w in widths),
            pltpu.VMEM((SEQ, D), BF16),
            pltpu.VMEM((SEQ, 640), F32),
            pltpu.VMEM((2 * LEVELS, SEQ, 2 * SEQ), BF16),
            pltpu.VMEM((SEQ, HEADS * SEQ), F32),
            pltpu.VMEM((SEQ, 256), BF16),
            pltpu.VMEM((SEQ, D), BF16),
            pltpu.VMEM((NTP, ROWS_OWN, D), BF16),
            pltpu.VMEM((SEQ, D), BF16),
            pltpu.VMEM((SEQ, 768), F32),
            pltpu.VMEM((SEQ, 384), BF16),
            pltpu.VMEM((SEQ, D), BF16),
            pltpu.VMEM((NTP, ROWS_OWN, D), BF16),
            pltpu.VMEM((ROWS_OWN, D), F32),
            pltpu.VMEM((2 * SEQ, 128), BF16),
            pltpu.VMEM((SEQ, 128), F32),
            pltpu.VMEM((SEQ, 128), F32),
            pltpu.VMEM((HEADS * SEQ, 256), BF16),
            pltpu.SemaphoreType.DMA((10,)),
            pltpu.SemaphoreType.DMA((4, 48)),
            pltpu.SemaphoreType.DMA((4, 48)),
            pltpu.SemaphoreType.DMA((4, NTP)),
            pltpu.SemaphoreType.DMA((4, NTP)),
        ],
        compiler_params=pltpu.CompilerParams(collective_id=0, has_side_effects=True),
    )(
        tokens,
        attention_norm_gain.reshape(1, D),
        decay_gate_bias.reshape(1, 128),
        decay_spike_extra.T,
        head_output_gain.reshape(1, VW),
        channel_norm_gain.reshape(1, D),
        query_weight, key_weight, value_weight, decay_weight, output_weight, gate_weight, up_weight, down_weight,
    )


def solution(mesh):
    rows, w = P(("rep", "fs"), None), P("fs", "tp")
    in_specs = (rows, P(), w, w, w, w, P("tp"), P(("rep", "fs"), "tp"), P(), w, P(), w, w, w)
    return jax.shard_map(shards, mesh=mesh, in_specs=in_specs, out_specs=rows, check_vma=False)
```

```python
import functools

import jax
import jax.numpy as jnp
from jax import lax
from jax.experimental import pallas as pl
from jax.experimental.pallas import tpu as pltpu
from jax.sharding import PartitionSpec as P

MESH = pl.DeviceIdType.MESH
F32, BF16 = jnp.float32, jnp.bfloat16
NY, NZ, NTP = 8, 4, 8
SEQ, D = 128, 2048
SLAB = D // (NY * NZ)
HEADS, KW, VW = 4, 32, 64
LEVELS = 7
EPS = 1e-6
PARTS = ((128, 128, 256, 128), (256,), (384, 384), (384,))
A_ROWS = (32, 32, 32, 48)
ROWS_OWN = SEQ // NTP


def messages(g):
    ra = A_ROWS[g]
    rows_a, rows_b = slice(0, ra), slice(ra, SLAB)
    half_a = (slice(0, 16 * ((ra // 16 + 1) // 2)), slice(16 * ((ra // 16 + 1) // 2), ra))
    half_b = (slice(ra, ra + 16 * ((SLAB - ra) // 32)), slice(ra + 16 * ((SLAB - ra) // 32), SLAB))
    out = {}
    for d in (0, 1):
        back = -1 if d == 0 else 1
        for s in range(4):
            out["ay", d, s] = ("y", 0, back * s, rows_a if s < 3 else half_a[d], (("ay", s - 1),) if s else (), ("ay", s))
        for i, off in enumerate((0, -1, 1, -2, 2, -3, 3, 4)):
            out["az", d, i] = ("z", 0, off, rows_a, (("ay", (i - 1) // 2),) if i else (), ("az", 0))
        out["az", d, 8] = ("z", back, slice(4 * d, 4 * d + 4), rows_a, (("az", 0),), ("az", 1))
        out["bz", d, 0] = ("z", 0, 0, rows_b, (), ("bz", 0))
        if half_b[d].stop > half_b[d].start:
            out["bz", d, 1] = ("z", back, 0, half_b[d], (("bz", 0),), ("bz", 1))
        for i, off in enumerate((0, -1, 1, 2)):
            out["by", d, i] = ("y", off, 0, rows_b, (("bz", i // 3),) if i else (), ("by", 0))
        for s in (1, 2):
            for h in (0, 1):
                half = slice(2 * h, 2 * h + 2)
                out["by", d, 2 + 2 * s + h] = (
                    "y", half, back * s, rows_b, (("by", 2 * s - 3 + h if s > 1 else 0),), ("by", 2 * s - 1 + h),
                )
        out["by", d, 8] = ("y", slice(2 * d, 2 * d + 2), back * 3, rows_b, (("by", 3 + d),), ("by", 5))
    return out


TAKES = [("ay", 0), ("ay", 1), ("ay", 2), ("ay", 3), ("az", 0), ("az", 1), ("bz", 0), ("bz", 1), *(("by", i) for i in range(6))]


def extent(i):
    return i.stop - i.start if isinstance(i, slice) else 1


def link_plan(near, ahead, hop=2.6, rate=46.6e3, turn=7.5, times=None):
    table = {(g, *m): v for g in range(4) for m, v in messages(g).items()}
    need = {m: {(m[0], *x) for x in v[4]} for m, v in table.items()}
    feeds, then = {}, {}
    for m, v in table.items():
        feeds.setdefault((m[0], *v[5]), set()).add(m)
        for x in need[m]:
            then.setdefault(x, []).append(m)

    def urgency(m):
        g, name, d, i = m
        second = name == "by" or name == "az"
        return (g * 10 - (0 if second else ahead), i, d)

    ready = {(a, d): [] for a in ("y", "z") for d in (0, 1)}
    free = dict.fromkeys(ready, 0.0)
    left = [sum(x[0] == g for x in feeds) for g in range(4)]
    for m, v in table.items():
        if not need[m]:
            ready[v[0], m[2]].append(m)
    now, ops, have, coming, at = 0.2, [], set(), [], 0
    landed = {}
    def fill(until):
        nonlocal now
        before = len(ops)
        for l, queue in ready.items():
            while queue and free[l] < until:
                m = min(queue, key=urgency)
                queue.remove(m)
                v = table[m]
                size = extent(v[1]) * extent(v[2]) * extent(v[3]) * sum(PARTS[m[0]]) * 2
                free[l] = max(now, free[l]) + size / rate
                landed[m] = free[l] + hop
                take = (m[0], *v[5])
                if all(x in landed for x in feeds[take]):
                    coming.append((max(landed[x] for x in feeds[take]), len(ops), take))
                ops.append(("send", m))
                now += 0.02
        return len(ops) > before

    while at < len(WORK) or coming:
        fill(now + near)
        coming.sort()
        if coming and coming[0][0] <= now:
            m = coming.pop(0)[2]
            ops.append(("take", m))
            now += 0.02
            if isinstance(m, str):
                have.add(m)
                continue
            left[m[0]] -= 1
            if left[m[0]] == 0:
                have.add(m[0])
                if times is not None:
                    times[m[0]] = now
            for x in then.get(m, ()):
                need[x].discard(m)
                if not need[x]:
                    ready[table[x][0], x[2]].append(x)
        elif at < len(WORK) and all(q in have for q in WORK[at][2]):
            name, span, _, gives = WORK[at]
            at += 1
            fill(now + span)
            now += span
            ops.append(("work", name))
            if gives:
                coming.append((now + turn, len(ops), gives))
        elif not fill(min(coming)[0] if coming else now + 1e3):
            now = max(now, min(coming)[0])
    if times is not None:
        times["end"] = now
    return ops


WORK = (
    ("norm", 0.92, (), None),
    ("mats", 0.42, (), None),
    ("project", 1.1, (0,), None),
    ("prepare", 0.27, (), None),
    *((f"level{l}", 0.34, (), None) for l in range(LEVELS)),
    ("attend", 0.5, (), None),
    ("mix_out", 0.9, (1,), "scatter1"),
    ("residual", 0.3, ("scatter1",), "spread1"),
    ("gate_up", 1.1, ("spread1", 2), None),
    ("hidden", 0.2, (), None),
    ("down", 1.1, (3,), "scatter2"),
    ("layer_out", 0.3, ("scatter2",), "spread2"),
    ("end", 0.1, ("spread2",), None),
)
NEAR, AHEAD = 0.5, 12


def dot(a, b):
    return jnp.dot(a, b, preferred_element_type=F32)


def dot_t(a, b):
    return lax.dot_general(a, b, (((1,), (1,)), ((), ())), preferred_element_type=F32)


def iota(shape, axis):
    return lax.broadcasted_iota(jnp.int32, shape, axis)


def layer_kernel(
    tok_hbm, gain1, bias, spike, hgain, gain2, wq, wk, wv, wd, wo, wg, wu, wdn,
    out,
    tok, extra, fin,
    g1, g2, g3, g4, xn, acc, mats, score, att, part, got, n2, acc2, hid, part2, got2, resid, decay2, qf, kf, vbd,
    lsem, send, recv, tsend, trecv,
):
    bufs = (g1, g2, g3, g4)
    rep, f, t = lax.axis_index("rep"), lax.axis_index("fs"), lax.axis_index("tp")
    y, z = lax.rem(f, NY), lax.div(f, NY)
    zz = rep * NZ + z

    def at_y(k):
        return (rep, z * NY + lax.rem(y + k + NY, NY), t)

    def at_z(k):
        w = lax.rem(zz + k + 2 * NZ, 2 * NZ)
        return (lax.div(w, NZ), lax.rem(w, NZ) * NY + y, t)

    ynb, znb = (at_y(1), at_y(-1)), (at_z(1), at_z(-1))

    def peer(k):
        return (rep, f, lax.rem(t + k, NTP))

    barrier = pltpu.get_barrier_semaphore()
    others = [*ynb, *znb, *(peer(k) for k in range(1, NTP))]
    for d in others:
        pl.semaphore_signal(barrier, inc=1, device_id=d, device_id_type=MESH)

    own = []
    srcs = ((wq, wk, wv, wd), (wo,), (wg, wu), (wdn,))
    for g in range(4):
        at, copies = 0, []
        for src, width in zip(srcs[g], PARTS[g]):
            copies.append(pltpu.make_async_copy(src, bufs[g].at[z, y, :, at : at + width], lsem.at[g]))
            at += width
        for c in copies:
            c.start()
        own.append(pltpu.make_async_copy(bufs[g].at[z, y], bufs[g].at[z, y], lsem.at[g]))
        if g == 0:
            tok_copy = pltpu.make_async_copy(tok_hbm, tok, lsem.at[4])
            tok_copy.start()

    pl.semaphore_wait(barrier, len(others))

    tables = [messages(g) for g in range(4)]

    def place(i, at, n):
        return i if isinstance(i, slice) else lax.rem(at + i + n, n)

    def send_weight(g, name, d, i):
        ring, zs, ys, rows, _, take = tables[g][name, d, i]
        ref = bufs[g].at[place(zs, z, NZ), place(ys, y, NY), rows, :]
        pltpu.make_async_remote_copy(
            src_ref=ref, dst_ref=ref, send_sem=send.at[g], recv_sem=recv.at[g, TAKES.index(take)],
            device_id=(ynb if ring == "y" else znb)[d], device_id_type=MESH,
        ).start()

    def wait_bytes(ref, sem):
        pltpu.make_async_copy(ref, ref, sem).wait()

    def take_weight(g, name, i):
        slabs, rows = 0, None
        for v in tables[g].values():
            if v[5] == (name, i):
                whole = extent(v[3])
                slabs += extent(v[1]) * extent(v[2]) * whole
        for nz, ny, size in ((1, 1, SLAB), (1, 2, SLAB), (1, 4, SLAB), (1, 8, SLAB), (2, 8, SLAB), (3, 8, SLAB)):
            if slabs % (nz * ny * 16) == 0 and slabs <= nz * ny * size:
                ref = bufs[g].at[0:nz, 0:ny, 0 : slabs // (nz * ny), :]
                wait_bytes(ref, recv.at[g, TAKES.index((name, i))])
                return
        raise ValueError(name)

    def norm_rows(i, c):
        r = pl.ds(pl.multiple_of(i * 16, 16), 16)
        v = tok[r, :].astype(F32)
        xn[r, :] = (v * lax.rsqrt(jnp.mean(v * v, axis=-1, keepdims=True) + EPS) * gain1[...]).astype(BF16)
        return c

    def norm():
        tok_copy.wait()
        lax.fori_loop(0, SEQ // 16, norm_rows, 0)

    def build_mats(l, c):
        ti, si = iota((SEQ, 2 * SEQ), 0), lax.rem(iota((SEQ, 2 * SEQ), 1), SEQ)
        same = lax.shift_right_logical(ti, l) == lax.shift_right_logical(si, l)
        back = (ti - si) * (2 * (lax.shift_right_logical(ti, l) & 1) - 1)
        mats[2 * l] = jnp.where(same & (back >= 0), 1.0, 0.0).astype(BF16)
        mats[2 * l + 1] = jnp.where(same & (back > 0), 1.0, 0.0).astype(BF16)
        return c

    def build():
        lax.fori_loop(0, LEVELS, build_mats, 0)
        heads = jnp.where(lax.div(iota((HEADS, 128), 1), KW) == iota((HEADS, 128), 0), 1.0, 0.0)
        extra[...] = lax.dot_general(
            spike[...], heads, (((0,), (0,)), ((), ())), precision=lax.Precision.HIGHEST, preferred_element_type=F32
        )

    def project():
        acc[...] = jnp.zeros_like(acc)

        def body(w, c):
            cols = pl.ds(pl.multiple_of(w * 512, 512), 512)
            acc[...] += dot(xn[:, cols], g1[w].reshape(512, 640))
            return c

        lax.fori_loop(0, NZ, body, 0)

    lane_head = lax.div(iota((SEQ, 128), 1), KW)

    def by_head(x):
        return jnp.concatenate([jnp.where(lane_head == h, x, 0.0).astype(BF16) for h in range(HEADS)], axis=0)

    def prepare():
        gate = acc[:, 512:640] + bias[...]
        logs = (jnp.minimum(gate, 0.0) - jnp.log1p(jnp.exp(-jnp.abs(gate)))) / 16.0 + extra[...]
        hi = logs.astype(BF16)
        decay2[0:SEQ, :] = hi
        decay2[SEQ : 2 * SEQ, :] = (logs - hi.astype(F32)).astype(BF16)
        qf[...] = acc[:, 0:128].astype(BF16).astype(F32)
        kf[...] = acc[:, 128:256].astype(BF16).astype(F32)
        vals = acc[:, 256:512]
        lane_vhead = lax.div(iota((SEQ, 256), 1), VW)
        for h in range(HEADS):
            vbd[h * SEQ : (h + 1) * SEQ, :] = jnp.where(lane_vhead == h, vals, 0.0).astype(BF16)
        score[...] = 2.0 * dot_t(qf[...].astype(BF16), by_head(kf[...]))

    def level(l):
        left = (qf[...] * jnp.exp(dot(mats[2 * l], decay2[...]))).astype(BF16)
        right = by_head(kf[...] * jnp.exp(dot(mats[2 * l + 1], decay2[...])))
        differ = iota((SEQ, HEADS * SEQ), 0) ^ lax.rem(iota((SEQ, HEADS * SEQ), 1), SEQ)
        score[...] = jnp.where(differ >= 2 ** l, dot_t(left, right), score[...])

    def attend():
        mixed = dot(score[...].astype(BF16), vbd[...]) * (KW ** -0.5)
        sq = mixed * mixed
        sq_hi = sq.astype(BF16)
        sq_lo = (sq - sq_hi.astype(F32)).astype(BF16)
        ones = jnp.where(lax.div(iota((256, 256), 0), VW) == lax.div(iota((256, 256), 1), VW), 1.0, 0.0).astype(BF16)
        mean = (dot(sq_hi, ones) + dot(sq_lo, ones)) * (1.0 / VW)
        gains = jnp.concatenate([hgain[...]] * HEADS, axis=1)
        att[...] = (mixed * lax.rsqrt(mean + EPS) * gains).astype(BF16)

    def project_out(left, weight, width, into):
        def body(w, c):
            cols = pl.ds(pl.multiple_of(w * 512, 512), 512)
            into[:, cols] = dot_t(left[...], weight[w].reshape(512, width)).astype(BF16)
            return c

        lax.fori_loop(0, NZ, body, 0)

    def rows_of(k):
        return pl.ds(pl.multiple_of(lax.rem(t + k + NTP, NTP) * ROWS_OWN, ROWS_OWN), ROWS_OWN)

    own_rows = rows_of(0)

    def exchange(n, k, src, dst):
        pltpu.make_async_remote_copy(
            src_ref=src, dst_ref=dst, send_sem=tsend.at[n], recv_sem=trecv.at[n],
            device_id=peer(k), device_id_type=MESH,
        ).start()

    def scatter(n, src, dst):
        for k in range(1, NTP):
            exchange(n, k, src.at[rows_of(k), :], dst.at[k])

    def spread(n, src, ref):
        for k in range(1, NTP):
            exchange(n, k, src, ref.at[own_rows, :])

    def exchange_wait(n, sem):
        wait_bytes(part.at[0 : SEQ - ROWS_OWN, :], sem.at[n])

    def total(src, dst):
        s = src[own_rows, :].astype(F32)
        for k in range(1, NTP):
            s = s + dst[k].astype(F32)
        return s

    def mix_out():
        project_out(att, g2, 256, part)
        scatter(0, part, got)

    def residual_rows():
        r = (tok[own_rows, :].astype(F32) + total(part, got)).astype(BF16).astype(F32)
        resid[...] = r
        n2[own_rows, :] = (r * lax.rsqrt(jnp.mean(r * r, axis=-1, keepdims=True) + EPS) * gain2[...]).astype(BF16)
        spread(1, n2.at[own_rows, :], n2)

    def gate_up():
        acc2[...] = jnp.zeros_like(acc2)

        def body(w, c):
            cols = pl.ds(pl.multiple_of(w * 512, 512), 512)
            acc2[...] += dot(n2[:, cols], g3[w].reshape(512, 768))
            return c

        lax.fori_loop(0, NZ, body, 0)

    def hidden():
        gated = acc2[:, 0:384]
        hid[...] = (gated / (1.0 + jnp.exp(-gated)) * acc2[:, 384:768]).astype(BF16)

    def down():
        project_out(hid, g4, 384, part2)
        scatter(2, part2, got2)

    own_out = pltpu.make_async_copy(fin, out.at[own_rows, :], lsem.at[5])

    def layer_out():
        fin[...] = (resid[...] + total(part2, got2)).astype(BF16)
        spread(3, fin, out)
        own_out.start()

    def end():
        own_out.wait()

    work = dict(
        norm=norm, mats=build, project=project, prepare=prepare, attend=attend, mix_out=mix_out,
        residual=residual_rows, gate_up=gate_up, hidden=hidden, down=down, layer_out=layer_out, end=end,
        **{f"level{l}": functools.partial(level, l) for l in range(LEVELS)},
    )
    turns = dict(scatter1=0, spread1=1, scatter2=2, spread2=3)
    waiting = set(range(4))
    for verb, what in link_plan(NEAR, AHEAD):
        with jax.named_scope(f"{verb}_{what}".replace(" ", "")):
            if verb == "work":
                work[what]()
            elif verb == "send":
                if what[0] in waiting:
                    waiting.discard(what[0])
                    own[what[0]].wait()
                send_weight(*what)
            elif isinstance(what, str):
                exchange_wait(turns[what], trecv)
            else:
                take_weight(*what)
    for g in range(4):
        wait_bytes(bufs[g].at[0:3], send.at[g])
        wait_bytes(bufs[g].at[3, 0:7], send.at[g])
        exchange_wait(g, tsend)


def shards(
    tokens, attention_norm_gain, query_weight, key_weight, value_weight, decay_weight, decay_gate_bias,
    decay_spike_extra, head_output_gain, output_weight, channel_norm_gain, gate_weight, up_weight, down_weight,
):
    vmem = pl.BlockSpec(memory_space=pltpu.VMEM)
    hbm = pl.BlockSpec(memory_space=pl.ANY)
    widths = [sum(p) for p in PARTS]
    return pl.pallas_call(
        layer_kernel,
        out_shape=jax.ShapeDtypeStruct((SEQ, D), BF16),
        in_specs=[hbm] + [vmem] * 5 + [hbm] * 8,
        out_specs=hbm,
        scratch_shapes=[
            pltpu.VMEM((SEQ, D), BF16),
            pltpu.VMEM((SEQ, 128), F32),
            pltpu.VMEM((ROWS_OWN, D), BF16),
            *(pltpu.VMEM((NZ, NY, SLAB, w), BF16) for w in widths),
            pltpu.VMEM((SEQ, D), BF16),
            pltpu.VMEM((SEQ, 640), F32),
            pltpu.VMEM((2 * LEVELS, SEQ, 2 * SEQ), BF16),
            pltpu.VMEM((SEQ, HEADS * SEQ), F32),
            pltpu.VMEM((SEQ, 256), BF16),
            pltpu.VMEM((SEQ, D), BF16),
            pltpu.VMEM((NTP, ROWS_OWN, D), BF16),
            pltpu.VMEM((SEQ, D), BF16),
            pltpu.VMEM((SEQ, 768), F32),
            pltpu.VMEM((SEQ, 384), BF16),
            pltpu.VMEM((SEQ, D), BF16),
            pltpu.VMEM((NTP, ROWS_OWN, D), BF16),
            pltpu.VMEM((ROWS_OWN, D), F32),
            pltpu.VMEM((2 * SEQ, 128), BF16),
            pltpu.VMEM((SEQ, 128), F32),
            pltpu.VMEM((SEQ, 128), F32),
            pltpu.VMEM((HEADS * SEQ, 256), BF16),
            pltpu.SemaphoreType.DMA((6,)),
            pltpu.SemaphoreType.DMA((4,)),
            pltpu.SemaphoreType.DMA((4, len(TAKES))),
            pltpu.SemaphoreType.DMA((4,)),
            pltpu.SemaphoreType.DMA((4,)),
        ],
        compiler_params=pltpu.CompilerParams(collective_id=0, has_side_effects=True),
    )(
        tokens,
        attention_norm_gain.reshape(1, D),
        decay_gate_bias.reshape(1, 128),
        decay_spike_extra.T,
        head_output_gain.reshape(1, VW),
        channel_norm_gain.reshape(1, D),
        query_weight, key_weight, value_weight, decay_weight, output_weight, gate_weight, up_weight, down_weight,
    )


def solution(mesh):
    rows, w = P(("rep", "fs"), None), P("fs", "tp")
    in_specs = (rows, P(), w, w, w, w, P("tp"), P(("rep", "fs"), "tp"), P(), w, P(), w, w, w)
    return jax.shard_map(shards, mesh=mesh, in_specs=in_specs, out_specs=rows, check_vma=False)
```

```python
import functools

import jax
import jax.numpy as jnp
from jax import lax
from jax.experimental import pallas as pl
from jax.experimental.pallas import tpu as pltpu
from jax.sharding import PartitionSpec as P

MESH = pl.DeviceIdType.MESH
F32, BF16 = jnp.float32, jnp.bfloat16
NY, NZ, NTP = 8, 4, 8
SEQ, D = 128, 2048
SLAB = D // (NY * NZ)
HEADS, KW, VW = 4, 32, 64
LEVELS = 7
EPS = 1e-6
PARTS = ((128, 128, 256, 128), (256,), (384, 384), (384,))
A_ROWS = (32, 32, 48, 32)
ROWS_OWN = SEQ // NTP


def messages(g):
    ra = A_ROWS[g]
    rows_a, rows_b = slice(0, ra), slice(ra, SLAB)
    half_a = (slice(0, 16 * ((ra // 16 + 1) // 2)), slice(16 * ((ra // 16 + 1) // 2), ra))
    half_b = (slice(ra, ra + 16 * ((SLAB - ra) // 32)), slice(ra + 16 * ((SLAB - ra) // 32), SLAB))
    out = {}
    for d in (0, 1):
        back = -1 if d == 0 else 1
        for s in range(4):
            out["ay", d, s] = ("y", 0, back * s, rows_a if s < 3 else half_a[d], (("ay", s - 1),) if s else (), ("ay", s))
        for i, off in enumerate((0, -1, 1, -2, 2, -3, 3, 4)):
            out["az", d, i] = ("z", 0, off, rows_a, (("ay", (i - 1) // 2),) if i else (), ("az", 0))
        out["az", d, 8] = ("z", back, slice(4 * d, 4 * d + 4), rows_a, (("az", 0),), ("az", 1))
        out["bz", d, 0] = ("z", 0, 0, rows_b, (), ("bz", 0))
        if half_b[d].stop > half_b[d].start:
            out["bz", d, 1] = ("z", back, 0, half_b[d], (("bz", 0),), ("bz", 1))
        for i, off in enumerate((0, -1, 1, 2)):
            out["by", d, i] = ("y", off, 0, rows_b, (("bz", i // 3),) if i else (), ("by", 0))
        for s in (1, 2):
            for h in (0, 1):
                half = slice(2 * h, 2 * h + 2)
                out["by", d, 2 + 2 * s + h] = (
                    "y", half, back * s, rows_b, (("by", 2 * s - 3 + h if s > 1 else 0),), ("by", 2 * s - 1 + h),
                )
        out["by", d, 8] = ("y", slice(2 * d, 2 * d + 2), back * 3, rows_b, (("by", 3 + d),), ("by", 5))
    return out


TAKES = [("ay", 0), ("ay", 1), ("ay", 2), ("ay", 3), ("az", 0), ("az", 1), ("bz", 0), ("bz", 1), *(("by", i) for i in range(6))]


def extent(i):
    return i.stop - i.start if isinstance(i, slice) else 1


def link_plan(near, ahead, hop=2.6, rate=46.6e3, times=None):
    table = {(g, *m): v for g in range(4) for m, v in messages(g).items()}
    need = {m: {(m[0], *x) for x in v[4]} for m, v in table.items()}
    feeds, then = {}, {}
    for m, v in table.items():
        feeds.setdefault((m[0], *v[5]), set()).add(m)
        for x in need[m]:
            then.setdefault(x, []).append(m)

    def urgency(m):
        g, name, d, i = m
        second = name == "by" or name == "az"
        return (g * 10 - (0 if second else ahead), i, d)

    ready = {(a, d): [] for a in ("y", "z") for d in (0, 1)}
    free = dict.fromkeys(ready, 0.0)
    left = [sum(x[0] == g for x in feeds) for g in range(4)]
    for m, v in table.items():
        if not need[m]:
            ready[v[0], m[2]].append(m)
    now, ops, have, coming, at = 0.2, [], set(), [], 0
    landed = {}
    def fill(until):
        nonlocal now
        before = len(ops)
        for l, queue in ready.items():
            while queue and free[l] < until:
                m = min(queue, key=urgency)
                queue.remove(m)
                v = table[m]
                size = extent(v[1]) * extent(v[2]) * extent(v[3]) * sum(PARTS[m[0]]) * 2
                free[l] = max(now, free[l]) + size / rate
                landed[m] = free[l] + hop
                take = (m[0], *v[5])
                if all(x in landed for x in feeds[take]):
                    coming.append((max(landed[x] for x in feeds[take]), len(ops), take))
                ops.append(("send", m))
                now += 0.02
        return len(ops) > before

    while at < len(WORK) or coming:
        fill(now + near)
        coming.sort()
        if coming and coming[0][0] <= now:
            m = coming.pop(0)[2]
            ops.append(("take", m))
            now += 0.02
            if isinstance(m, str):
                have.add(m)
                continue
            left[m[0]] -= 1
            if left[m[0]] == 0:
                have.add(m[0])
                if times is not None:
                    times[m[0]] = now
            for x in then.get(m, ()):
                need[x].discard(m)
                if not need[x]:
                    ready[table[x][0], x[2]].append(x)
        elif at < len(WORK) and all(q in have for q in WORK[at][2]):
            name, span, _, gives = WORK[at]
            at += 1
            fill(now + span)
            now += span
            ops.append(("work", name))
            coming.extend((now + TURN[x[0]], len(ops), x) for x in gives)
        elif not fill(min(coming)[0] if coming else now + 1e3):
            now = max(now, min(coming)[0])
    if times is not None:
        times["end"] = now
    return ops


WORK = (
    ("norm", 0.92, (), ()),
    ("mats", 0.67, (), ()),
    ("project", 1.1, (0,), ()),
    ("prepare", 0.27, (), ()),
    *((f"level{l}", 0.34, (), ()) for l in range(LEVELS)),
    ("attend", 0.35, (), ()),
    ("mix0", 0.5, (1,), ("d00",)),
    ("mix1", 0.5, (), ("d01",)),
    ("pair00", 0.1, ("d00",), ("x00",)),
    ("pair01", 0.1, ("d01",), ("x01",)),
    ("residual", 0.25, ("x00", "x01"), ("s00", "s01")),
    ("relay00", 0.05, ("s00",), ("f00",)),
    ("relay01", 0.05, ("s01",), ("f01",)),
    ("gate_up", 1.1, ("f00", "f01", 2), ()),
    ("hidden", 0.07, (), ()),
    ("down0", 0.53, (3,), ("d10",)),
    ("down1", 0.53, (), ("d11",)),
    ("pair10", 0.1, ("d10",), ("x10",)),
    ("pair11", 0.1, ("d11",), ("x11",)),
    ("layer0", 0.1, ("x10",), ("s10",)),
    ("layer1", 0.1, ("x11",), ("s11",)),
    ("relay10", 0.05, ("s10",), ("f10",)),
    ("relay11", 0.05, ("s11",), ("f11",)),
    ("end", 0.1, ("f10", "f11"), ()),
)
TURN = dict(d=1.4, x=4.6, s=4.6, f=1.4)
NEAR, AHEAD = 0.5, 12


def dot(a, b):
    return jnp.dot(a, b, preferred_element_type=F32)


def dot_t(a, b):
    return lax.dot_general(a, b, (((1,), (1,)), ((), ())), preferred_element_type=F32)


def iota(shape, axis):
    return lax.broadcasted_iota(jnp.int32, shape, axis)


def layer_kernel(
    tok_hbm, gain1, bias, spike, hgain, gain2, wq, wk, wv, wd, wo, wg, wu, wdn,
    out,
    tok, extra, fin,
    g1, g2, g3, g4, xn, acc, mats, score, att, n2, acc2, hid, resid, decay2, qf, kf, vbd,
    part, part2, land, land2, both1, both2, got, got2,
    lsem, send, recv, tsend, trecv,
):
    bufs = (g1, g2, g3, g4)
    parts, lands, both, gots = (part, part2), (land, land2), (both1, both2), (got, got2)
    rep, f, t = lax.axis_index("rep"), lax.axis_index("fs"), lax.axis_index("tp")
    y, z = lax.rem(f, NY), lax.div(f, NY)
    zz = rep * NZ + z

    def at_y(k):
        return (rep, z * NY + lax.rem(y + k + NY, NY), t)

    def at_z(k):
        w = lax.rem(zz + k + 2 * NZ, 2 * NZ)
        return (lax.div(w, NZ), lax.rem(w, NZ) * NY + y, t)

    ynb, znb = (at_y(1), at_y(-1)), (at_z(1), at_z(-1))

    x, core = lax.div(t, 2), lax.rem(t, 2)
    partner = (rep, f, t + 1 - 2 * core)

    def around(k):
        return lax.rem(x + k, NTP // 2)

    def peer(k):
        return (rep, f, 2 * around(k) + core)

    barrier = pltpu.get_barrier_semaphore()
    others = [*ynb, *znb, partner, *(peer(k) for k in (1, 2, 3))]
    for d in others:
        pl.semaphore_signal(barrier, inc=1, device_id=d, device_id_type=MESH)

    own = []
    srcs = ((wq, wk, wv, wd), (wo,), (wg, wu), (wdn,))
    for g in range(4):
        at, copies = 0, []
        for src, width in zip(srcs[g], PARTS[g]):
            copies.append(pltpu.make_async_copy(src, bufs[g].at[z, y, :, at : at + width], lsem.at[g]))
            at += width
        for c in copies:
            c.start()
        own.append(pltpu.make_async_copy(bufs[g].at[z, y], bufs[g].at[z, y], lsem.at[g]))
        if g == 0:
            tok_copy = pltpu.make_async_copy(tok_hbm, tok, lsem.at[4])
            tok_copy.start()

    pl.semaphore_wait(barrier, len(others))

    tables = [messages(g) for g in range(4)]

    def place(i, at, n):
        return i if isinstance(i, slice) else lax.rem(at + i + n, n)

    def send_weight(g, name, d, i):
        ring, zs, ys, rows, _, take = tables[g][name, d, i]
        ref = bufs[g].at[place(zs, z, NZ), place(ys, y, NY), rows, :]
        pltpu.make_async_remote_copy(
            src_ref=ref, dst_ref=ref, send_sem=send.at[g], recv_sem=recv.at[g, TAKES.index(take)],
            device_id=(ynb if ring == "y" else znb)[d], device_id_type=MESH,
        ).start()

    def wait_bytes(ref, sem):
        pltpu.make_async_copy(ref, ref, sem).wait()

    def take_weight(g, name, i):
        slabs, rows = 0, None
        for v in tables[g].values():
            if v[5] == (name, i):
                whole = extent(v[3])
                slabs += extent(v[1]) * extent(v[2]) * whole
        for nz, ny, size in ((1, 1, SLAB), (1, 2, SLAB), (1, 4, SLAB), (1, 8, SLAB), (2, 8, SLAB), (3, 8, SLAB)):
            if slabs % (nz * ny * 16) == 0 and slabs <= nz * ny * size:
                ref = bufs[g].at[0:nz, 0:ny, 0 : slabs // (nz * ny), :]
                wait_bytes(ref, recv.at[g, TAKES.index((name, i))])
                return
        raise ValueError(name)

    def norm_rows(i, c):
        r = pl.ds(pl.multiple_of(i * 16, 16), 16)
        v = tok[r, :].astype(F32)
        xn[r, :] = (v * lax.rsqrt(jnp.mean(v * v, axis=-1, keepdims=True) + EPS) * gain1[...]).astype(BF16)
        return c

    def norm():
        tok_copy.wait()
        lax.fori_loop(0, SEQ // 16, norm_rows, 0)

    def build_mats(l, c):
        ti, si = iota((SEQ, 2 * SEQ), 0), lax.rem(iota((SEQ, 2 * SEQ), 1), SEQ)
        same = lax.shift_right_logical(ti, l) == lax.shift_right_logical(si, l)
        back = (ti - si) * (2 * (lax.shift_right_logical(ti, l) & 1) - 1)
        mats[2 * l] = jnp.where(same & (back >= 0), 1.0, 0.0).astype(BF16)
        mats[2 * l + 1] = jnp.where(same & (back > 0), 1.0, 0.0).astype(BF16)
        return c

    def build():
        lax.fori_loop(0, LEVELS, build_mats, 0)
        heads = jnp.where(lax.div(iota((HEADS, 128), 1), KW) == iota((HEADS, 128), 0), 1.0, 0.0)
        extra[...] = lax.dot_general(
            spike[...], heads, (((0,), (0,)), ((), ())), precision=lax.Precision.HIGHEST, preferred_element_type=F32
        )

    def project():
        acc[...] = jnp.zeros_like(acc)

        def body(w, c):
            cols = pl.ds(pl.multiple_of(w * 512, 512), 512)
            acc[...] += dot(xn[:, cols], g1[w].reshape(512, 640))
            return c

        lax.fori_loop(0, NZ, body, 0)

    lane_head = lax.div(iota((SEQ, 128), 1), KW)

    def by_head(x):
        return jnp.concatenate([jnp.where(lane_head == h, x, 0.0).astype(BF16) for h in range(HEADS)], axis=0)

    def prepare():
        gate = acc[:, 512:640] + bias[...]
        logs = (jnp.minimum(gate, 0.0) - jnp.log1p(jnp.exp(-jnp.abs(gate)))) / 16.0 + extra[...]
        hi = logs.astype(BF16)
        decay2[0:SEQ, :] = hi
        decay2[SEQ : 2 * SEQ, :] = (logs - hi.astype(F32)).astype(BF16)
        qf[...] = acc[:, 0:128].astype(BF16).astype(F32)
        kf[...] = acc[:, 128:256].astype(BF16).astype(F32)
        vals = acc[:, 256:512]
        lane_vhead = lax.div(iota((SEQ, 256), 1), VW)
        for h in range(HEADS):
            vbd[h * SEQ : (h + 1) * SEQ, :] = jnp.where(lane_vhead == h, vals, 0.0).astype(BF16)
        score[...] = 2.0 * dot_t(qf[...].astype(BF16), by_head(kf[...]))

    def level(l):
        left = (qf[...] * jnp.exp(dot(mats[2 * l], decay2[...]))).astype(BF16)
        right = by_head(kf[...] * jnp.exp(dot(mats[2 * l + 1], decay2[...])))
        differ = iota((SEQ, HEADS * SEQ), 0) ^ lax.rem(iota((SEQ, HEADS * SEQ), 1), SEQ)
        score[...] = jnp.where(differ >= 2 ** l, dot_t(left, right), score[...])

    def attend():
        mixed = dot(score[...].astype(BF16), vbd[...]) * (KW ** -0.5)
        sq = mixed * mixed
        sq_hi = sq.astype(BF16)
        sq_lo = (sq - sq_hi.astype(F32)).astype(BF16)
        ones = jnp.where(lax.div(iota((256, 256), 0), VW) == lax.div(iota((256, 256), 1), VW), 1.0, 0.0).astype(BF16)
        mean = (dot(sq_hi, ones) + dot(sq_lo, ones)) * (1.0 / VW)
        gains = jnp.concatenate([hgain[...]] * HEADS, axis=1)
        att[...] = (mixed * lax.rsqrt(mean + EPS) * gains).astype(BF16)

    def cols_of(c):
        return slice(c * D // 2, (c + 1) * D // 2)

    def copy_to(device, n, src, dst, sem):
        pltpu.make_async_remote_copy(
            src_ref=src, dst_ref=dst, send_sem=tsend.at[n], recv_sem=sem, device_id=device, device_id_type=MESH
        ).start()

    def project_out(n, c, left, weight, width):
        into = parts[n]

        def body(w, carry):
            cols = pl.ds(pl.multiple_of(w * 512, 512), 512)
            value = dot_t(left[...], weight[w].reshape(512, width)).astype(BF16)
            into[:, :, :, cols] = value.reshape(NTP // 2, 2, ROWS_OWN, 512)
            return carry

        lax.fori_loop(2 * c, 2 * c + 2, body, 0)
        cols = cols_of(c)
        copy_to(partner, n, into.at[:, 1 - core, :, cols], lands[n].at[:, :, cols], trecv.at[n, 0, c])

    def pair(n, c):
        cols = cols_of(c)
        both[n][:, :, cols] = (
            parts[n][:, core, :, cols].astype(F32) + lands[n][:, :, cols].astype(F32)
        ).astype(BF16)
        for k in (1, 2, 3):
            copy_to(peer(k), n, both[n].at[around(k), :, cols], gots[n].at[k - 1, :, cols], trecv.at[n, 1, c])

    def total(n, cols):
        s = parts[n][x, core, :, cols].astype(F32) + lands[n][x, :, cols].astype(F32)
        for k in range(3):
            s = s + gots[n][k, :, cols].astype(F32)
        return s

    own_rows = pl.ds(pl.multiple_of(t * ROWS_OWN, ROWS_OWN), ROWS_OWN)

    def residual_rows():
        r = (tok[own_rows, :].astype(F32) + total(0, slice(0, D))).astype(BF16).astype(F32)
        resid[...] = r
        n2[x, core] = (r * lax.rsqrt(jnp.mean(r * r, axis=-1, keepdims=True) + EPS) * gain2[...]).astype(BF16)
        for c in (0, 1):
            mine = n2.at[x, core, :, cols_of(c)]
            for k in (1, 2, 3):
                copy_to(peer(k), 0, mine, mine, trecv.at[0, 2, c])
            copy_to(partner, 0, mine, mine, trecv.at[0, 3, c])

    def relay_normed(c):
        for k in (1, 2, 3):
            piece = n2.at[around(k), core, :, cols_of(c)]
            copy_to(partner, 0, piece, piece, trecv.at[0, 3, c])

    def out_at(i, c):
        rows = pl.ds(pl.multiple_of((2 * i + core) * ROWS_OWN, ROWS_OWN), ROWS_OWN)
        return out.at[rows, cols_of(c)]

    def put(i, c):
        piece = fin.at[i, :, cols_of(c)]
        copy_to(partner, 1, piece, out_at(i, c), trecv.at[1, 3, c])
        pltpu.make_async_copy(piece, out_at(i, c), lsem.at[5]).start()

    def layer_out(c):
        cols = cols_of(c)
        fin[x, :, cols] = (resid[:, cols] + total(1, cols)).astype(BF16)
        for k in (1, 2, 3):
            copy_to(peer(k), 1, fin.at[x, :, cols], fin.at[x, :, cols], trecv.at[1, 2, c])
        put(x, c)

    def relay_out(c):
        for k in (1, 2, 3):
            put(around(k), c)

    def end():
        wait_bytes(fin, lsem.at[5])

    def take_exchange(what):
        n, c = int(what[1]), int(what[2])
        kind = "dxsf".index(what[0])
        ref = lands[n].at[:, :, cols_of(c)] if what[0] in "df" else gots[n].at[:, :, cols_of(c)]
        wait_bytes(ref, trecv.at[n, kind, c])

    def gate_up():
        acc2[...] = jnp.zeros_like(acc2)

        def body(w, c):
            cols = pl.ds(pl.multiple_of(w * 512, 512), 512)
            acc2[...] += dot(n2[:, :, :, cols].reshape(SEQ, 512), g3[w].reshape(512, 768))
            return c

        lax.fori_loop(0, NZ, body, 0)

    def hidden():
        gated = acc2[:, 0:384]
        hid[...] = (gated / (1.0 + jnp.exp(-gated)) * acc2[:, 384:768]).astype(BF16)

    work = dict(
        norm=norm, mats=build, project=project, prepare=prepare, attend=attend,
        residual=residual_rows, gate_up=gate_up, hidden=hidden, end=end,
        **{f"level{l}": functools.partial(level, l) for l in range(LEVELS)},
        **{f"pair{n}{c}": functools.partial(pair, n, c) for n in (0, 1) for c in (0, 1)},
    )
    for c in (0, 1):
        work[f"mix{c}"] = functools.partial(project_out, 0, c, att, g2, 256)
        work[f"down{c}"] = functools.partial(project_out, 1, c, hid, g4, 384)
        work[f"relay0{c}"] = functools.partial(relay_normed, c)
        work[f"relay1{c}"] = functools.partial(relay_out, c)
        work[f"layer{c}"] = functools.partial(layer_out, c)
    waiting = set(range(4))
    for verb, what in link_plan(NEAR, AHEAD):
        with jax.named_scope(f"{verb}_{what}".replace(" ", "")):
            if verb == "work":
                work[what]()
            elif verb == "send":
                if what[0] in waiting:
                    waiting.discard(what[0])
                    own[what[0]].wait()
                send_weight(*what)
            elif isinstance(what, str):
                take_exchange(what)
            else:
                take_weight(*what)
    for g in range(4):
        wait_bytes(bufs[g].at[0:3], send.at[g])
        wait_bytes(bufs[g].at[3, 0:7], send.at[g])
    for n in (0, 1):
        wait_bytes(parts[n], tsend.at[n])
        wait_bytes(parts[n].at[0:3], tsend.at[n])


def shards(
    tokens, attention_norm_gain, query_weight, key_weight, value_weight, decay_weight, decay_gate_bias,
    decay_spike_extra, head_output_gain, output_weight, channel_norm_gain, gate_weight, up_weight, down_weight,
):
    vmem = pl.BlockSpec(memory_space=pltpu.VMEM)
    hbm = pl.BlockSpec(memory_space=pl.ANY)
    widths = [sum(p) for p in PARTS]
    return pl.pallas_call(
        layer_kernel,
        out_shape=jax.ShapeDtypeStruct((SEQ, D), BF16),
        in_specs=[hbm] + [vmem] * 5 + [hbm] * 8,
        out_specs=hbm,
        scratch_shapes=[
            pltpu.VMEM((SEQ, D), BF16),
            pltpu.VMEM((SEQ, 128), F32),
            pltpu.VMEM((NTP // 2, ROWS_OWN, D), BF16),
            *(pltpu.VMEM((NZ, NY, SLAB, w), BF16) for w in widths),
            pltpu.VMEM((SEQ, D), BF16),
            pltpu.VMEM((SEQ, 640), F32),
            pltpu.VMEM((2 * LEVELS, SEQ, 2 * SEQ), BF16),
            pltpu.VMEM((SEQ, HEADS * SEQ), F32),
            pltpu.VMEM((SEQ, 256), BF16),
            pltpu.VMEM((NTP // 2, 2, ROWS_OWN, D), BF16),
            pltpu.VMEM((SEQ, 768), F32),
            pltpu.VMEM((SEQ, 384), BF16),
            pltpu.VMEM((ROWS_OWN, D), F32),
            pltpu.VMEM((2 * SEQ, 128), BF16),
            pltpu.VMEM((SEQ, 128), F32),
            pltpu.VMEM((SEQ, 128), F32),
            pltpu.VMEM((HEADS * SEQ, 256), BF16),
            *[pltpu.VMEM((NTP // 2, 2, ROWS_OWN, D), BF16)] * 2,
            *[pltpu.VMEM((NTP // 2, ROWS_OWN, D), BF16)] * 4,
            *[pltpu.VMEM((NTP // 2 - 1, ROWS_OWN, D), BF16)] * 2,
            pltpu.SemaphoreType.DMA((6,)),
            pltpu.SemaphoreType.DMA((4,)),
            pltpu.SemaphoreType.DMA((4, len(TAKES))),
            pltpu.SemaphoreType.DMA((2,)),
            pltpu.SemaphoreType.DMA((2, 4, 2)),
        ],
        compiler_params=pltpu.CompilerParams(collective_id=0, has_side_effects=True),
    )(
        tokens,
        attention_norm_gain.reshape(1, D),
        decay_gate_bias.reshape(1, 128),
        decay_spike_extra.T,
        head_output_gain.reshape(1, VW),
        channel_norm_gain.reshape(1, D),
        query_weight, key_weight, value_weight, decay_weight, output_weight, gate_weight, up_weight, down_weight,
    )


def solution(mesh):
    rows, w = P(("rep", "fs"), None), P("fs", "tp")
    in_specs = (rows, P(), w, w, w, w, P("tp"), P(("rep", "fs"), "tp"), P(), w, P(), w, w, w)
    return jax.shard_map(shards, mesh=mesh, in_specs=in_specs, out_specs=rows, check_vma=False)
```

```python
import functools

import jax
import jax.numpy as jnp
from jax import lax
from jax.experimental import pallas as pl
from jax.experimental.pallas import tpu as pltpu
from jax.sharding import PartitionSpec as P

MESH = pl.DeviceIdType.MESH
F32, BF16 = jnp.float32, jnp.bfloat16
NY, NZ, NTP = 8, 4, 8
SEQ, D = 128, 2048
SLAB = D // (NY * NZ)
HEADS, KW, VW = 4, 32, 64
LEVELS = 7
EPS = 1e-6
PARTS = ((128, 128, 256, 128), (256,), (384, 384), (384,))
A_ROWS = (32, 48, 32, 64)
ROWS_OWN = SEQ // NTP
CHUNKS = NZ
SLAB_ORDER = (0, -1, 1, 2)


def messages(g):
    ra = A_ROWS[g]
    rows_a, rows_b = slice(0, ra), slice(ra, SLAB)
    half_a = (slice(0, 16 * ((ra // 16 + 1) // 2)), slice(16 * ((ra // 16 + 1) // 2), ra))
    half_b = (slice(ra, ra + 16 * ((SLAB - ra) // 32)), slice(ra + 16 * ((SLAB - ra) // 32), SLAB))
    out = {}
    for d in (0, 1):
        back = -1 if d == 0 else 1
        for s in range(4):
            out["ay", d, s] = ("y", 0, back * s, rows_a if s < 3 else half_a[d], (("ay", s - 1),) if s else (), ("ay", s))
        for i, off in enumerate((0, -1, 1, -2, 2, -3, 3, 4)):
            out["az", d, i] = ("z", 0, off, rows_a, (("ay", (i - 1) // 2),) if i else (), ("az", 0))
        out["az", d, 8] = ("z", back, slice(4 * d, 4 * d + 4), rows_a, (("az", 0),), ("az", 1))
        out["bz", d, 0] = ("z", 0, 0, rows_b, (), ("bz", 0))
        if half_b[d].stop > half_b[d].start:
            out["bz", d, 1] = ("z", back, 0, half_b[d], (("bz", 0),), ("bz", 1))
        for i, off in enumerate((0, -1, 1, 2)):
            out["by", d, i] = ("y", off, 0, rows_b, (("bz", i // 3),) if i else (), ("by", 0))
        for s in (1, 2):
            for h in (0, 1):
                half = slice(2 * h, 2 * h + 2)
                out["by", d, 2 + 2 * s + h] = (
                    "y", half, back * s, rows_b, (("by", 2 * s - 3 + h if s > 1 else 0),), ("by", 2 * s - 1 + h),
                )
        out["by", d, 8] = ("y", slice(2 * d, 2 * d + 2), back * 3, rows_b, (("by", 3 + d),), ("by", 5))
    return {m: v for m, v in out.items() if extent(v[3])}


TAKES = [("ay", 0), ("ay", 1), ("ay", 2), ("ay", 3), ("az", 0), ("az", 1), ("bz", 0), ("bz", 1), *(("by", i) for i in range(6))]


def extent(i):
    return i.stop - i.start if isinstance(i, slice) else 1


def link_plan(near, hop=2.4, rate=46.6e3, times=None):
    table = {(g, *m): v for g in range(4) for m, v in messages(g).items()}
    need = {m: {(m[0], *x) for x in v[4]} for m, v in table.items()}
    feeds, then = {}, {}
    for m, v in table.items():
        feeds.setdefault((m[0], *v[5]), set()).add(m)
        for x in need[m]:
            then.setdefault(x, []).append(m)

    def urgency(m):
        g, name, d, i = m
        second = name == "by" or name == "az"
        return (BASE[g] if second else LIGHT[g], i, d)

    ready = {(a, d): [] for a in ("y", "z") for d in (0, 1)}
    free = dict.fromkeys(ready, 0.0)
    left = [sum(x[0] == g for x in feeds) for g in range(4)]
    for m, v in table.items():
        if not need[m]:
            ready[v[0], m[2]].append(m)
    now, ops, have, coming, todo = 0.2, [], set(), [], list(WORK)
    landed = {}
    def fill(until):
        nonlocal now
        before = len(ops)
        for l, queue in ready.items():
            while queue and free[l] < until:
                m = min(queue, key=urgency)
                queue.remove(m)
                v = table[m]
                size = extent(v[1]) * extent(v[2]) * extent(v[3]) * sum(PARTS[m[0]]) * 2
                free[l] = max(now, free[l]) + size / rate
                landed[m] = free[l] + hop
                take = (m[0], *v[5])
                if all(x in landed for x in feeds[take]):
                    coming.append((max(landed[x] for x in feeds[take]), len(ops), take))
                ops.append(("send", m))
                now += 0.02
        return len(ops) > before

    while todo or coming:
        fill(now + near)
        coming.sort()
        if coming and coming[0][0] <= now:
            m = coming.pop(0)[2]
            ops.append(("take", m))
            now += 0.02
            have.add(m)
            if isinstance(m, str):
                continue
            left[m[0]] -= 1
            if left[m[0]] == 0:
                have.add(m[0])
                if times is not None:
                    times[m[0]] = now
            for x in then.get(m, ()):
                need[x].discard(m)
                if not need[x]:
                    ready[table[x][0], x[2]].append(x)
            continue
        item = next((w for w in todo if all(q in have for q in w[2])), None)
        if item:
            todo.remove(item)
            name, span, _, gives = item
            have.add(name)
            fill(now + span)
            now += span
            ops.append(("work", name))
            coming.extend((now + TURN[x[0]], len(ops), x) for x in gives)
        elif not fill(min(coming)[0] if coming else now + 1e3):
            now = max(now, min(coming)[0])
    if times is not None:
        times["end"] = now
    return ops


EACH = range(CHUNKS)
LAST = ((3, "ay", 0), (3, "ay", 1), (3, "ay", 2), (3, "ay", 3)), ((3, "az", 0),), ((3, "az", 0),), ((3, "az", 1),)
WORK = (
    ("norm", 0.92, (), ()),
    ("mats", 0.67, (), ()),
    ("project", 1.1, ("norm", 0), ()),
    ("prepare", 0.27, ("project", "mats"), ()),
    *((f"level{l}", 0.34, (f"level{l - 1}" if l else "prepare",), ()) for l in range(LEVELS)),
    ("attend", 0.36, (f"level{LEVELS - 1}",), ()),
    *((f"mix{c}", 0.23, ("attend", 1), (f"d0{c}",)) for c in EACH),
    *((f"pair0{c}", 0.05, (f"d0{c}",), (f"x0{c}",)) for c in EACH),
    ("residual", 0.2, tuple(f"x0{c}" for c in EACH), tuple(f"s0{c}" for c in EACH)),
    *((f"relay0{c}", 0.03, (f"s0{c}",), (f"f0{c}",)) for c in EACH),
    ("gate_up", 1.12, (*(f"f0{c}" for c in EACH), *(f"relay0{c}" for c in EACH), 2), ()),
    ("hidden", 0.07, ("gate_up",), ()),
    *((f"down{c}", 0.27, ("hidden", *LAST[c]), (f"d1{c}",)) for c in EACH),
    *((f"pair1{c}", 0.05, (f"d1{c}",), (f"x1{c}",)) for c in EACH),
    *((f"layer{c}", 0.05, (f"x1{c}",), (f"s1{c}",)) for c in EACH),
    *((f"relay1{c}", 0.03, (f"s1{c}",), (f"f1{c}",)) for c in EACH),
    ("end", 0.1, (*(f"f1{c}" for c in EACH), *(f"relay1{c}" for c in EACH)), ()),
)
TURN = dict(d=1.3, x=4.9, s=4.4, f=1.3)
NEAR = 0.3
BASE, LIGHT = (0, -1, 20, 22), (-12, -13, 2, 19)


def dot(a, b):
    return jnp.dot(a, b, preferred_element_type=F32)


def dot_t(a, b):
    return lax.dot_general(a, b, (((1,), (1,)), ((), ())), preferred_element_type=F32)


def iota(shape, axis):
    return lax.broadcasted_iota(jnp.int32, shape, axis)


def layer_kernel(
    tok_hbm, gain1_hbm, bias_hbm, spike_hbm, hgain_hbm, gain2_hbm, wq, wk, wv, wd, wo, wg, wu, wdn,
    out,
    tok, gain1, bias, spike, hgain, gain2, extra, fin,
    g1, g2, g3, g4, xn, acc, mats, score, att, n2, acc2, hid, resid, decay2, qf, kf, vbd,
    part, part2, land, land2, both1, both2, got, got2,
    lsem, send, recv, tsend, trecv,
):
    bufs = (g1, g2, g3, g4)
    parts, lands, both, gots = (part, part2), (land, land2), (both1, both2), (got, got2)
    rep, f, t = lax.axis_index("rep"), lax.axis_index("fs"), lax.axis_index("tp")
    y, z = lax.rem(f, NY), lax.div(f, NY)
    zz = rep * NZ + z

    def at_y(k):
        return (rep, z * NY + lax.rem(y + k + NY, NY), t)

    def at_z(k):
        w = lax.rem(zz + k + 2 * NZ, 2 * NZ)
        return (lax.div(w, NZ), lax.rem(w, NZ) * NY + y, t)

    ynb, znb = (at_y(1), at_y(-1)), (at_z(1), at_z(-1))

    x, core = lax.div(t, 2), lax.rem(t, 2)
    partner = (rep, f, t + 1 - 2 * core)

    def around(k):
        return lax.rem(x + k, NTP // 2)

    def peer(k):
        return (rep, f, 2 * around(k) + core)

    barrier = pltpu.get_barrier_semaphore()
    others = [*ynb, *znb, partner, *(peer(k) for k in (1, 2, 3))]
    for d in others:
        pl.semaphore_signal(barrier, inc=1, device_id=d, device_id_type=MESH)

    own = []
    srcs = ((wq, wk, wv, wd), (wo,), (wg, wu), (wdn,))
    for g in range(4):
        at, copies = 0, []
        for src, width in zip(srcs[g], PARTS[g]):
            copies.append(pltpu.make_async_copy(src, bufs[g].at[z, y, :, at : at + width], lsem.at[g]))
            at += width
        for c in copies:
            c.start()
        own.append(pltpu.make_async_copy(bufs[g].at[z, y], bufs[g].at[z, y], lsem.at[g]))
        if g == 0:
            small = ((gain1_hbm, gain1), (bias_hbm, bias), (spike_hbm, spike), (hgain_hbm, hgain), (gain2_hbm, gain2))
            fetches = [
                pltpu.make_async_copy(src, dst, lsem.at[6 + i]) for i, (src, dst) in enumerate(((tok_hbm, tok), *small))
            ]
            for c in fetches:
                c.start()

    pl.semaphore_wait(barrier, len(others))

    tables = [messages(g) for g in range(4)]

    def place(i, at, n):
        return i if isinstance(i, slice) else lax.rem(at + i + n, n)

    def send_weight(g, name, d, i):
        ring, zs, ys, rows, _, take = tables[g][name, d, i]
        ref = bufs[g].at[place(zs, z, NZ), place(ys, y, NY), rows, :]
        pltpu.make_async_remote_copy(
            src_ref=ref, dst_ref=ref, send_sem=send.at[g], recv_sem=recv.at[g, TAKES.index(take)],
            device_id=(ynb if ring == "y" else znb)[d], device_id_type=MESH,
        ).start()

    def wait_bytes(ref, sem):
        pltpu.make_async_copy(ref, ref, sem).wait()

    def take_weight(g, name, i):
        slabs, rows = 0, None
        for v in tables[g].values():
            if v[5] == (name, i):
                whole = extent(v[3])
                slabs += extent(v[1]) * extent(v[2]) * whole
        for nz, ny, size in ((1, 1, SLAB), (1, 2, SLAB), (1, 4, SLAB), (1, 8, SLAB), (2, 8, SLAB), (3, 8, SLAB)):
            if slabs % (nz * ny * 16) == 0 and slabs <= nz * ny * size:
                ref = bufs[g].at[0:nz, 0:ny, 0 : slabs // (nz * ny), :]
                wait_bytes(ref, recv.at[g, TAKES.index((name, i))])
                return
        raise ValueError(name)

    def norm_rows(i, c):
        r = pl.ds(pl.multiple_of(i * 16, 16), 16)
        v = tok[r, :].astype(F32)
        xn[r, :] = (v * lax.rsqrt(jnp.mean(v * v, axis=-1, keepdims=True) + EPS) * gain1[...]).astype(BF16)
        return c

    def norm():
        for c in fetches:
            c.wait()
        lax.fori_loop(0, SEQ // 16, norm_rows, 0)

    def build_mats(l, c):
        ti, si = iota((SEQ, 2 * SEQ), 0), lax.rem(iota((SEQ, 2 * SEQ), 1), SEQ)
        same = lax.shift_right_logical(ti, l) == lax.shift_right_logical(si, l)
        back = (ti - si) * (2 * (lax.shift_right_logical(ti, l) & 1) - 1)
        mats[2 * l] = jnp.where(same & (back >= 0), 1.0, 0.0).astype(BF16)
        mats[2 * l + 1] = jnp.where(same & (back > 0), 1.0, 0.0).astype(BF16)
        return c

    def build():
        lax.fori_loop(0, LEVELS, build_mats, 0)
        heads = jnp.where(lax.div(iota((HEADS, 128), 1), KW) == iota((HEADS, 128), 0), 1.0, 0.0)
        extra[...] = lax.dot_general(
            spike[...], heads, (((0,), (0,)), ((), ())), precision=lax.Precision.HIGHEST, preferred_element_type=F32
        )

    def project():
        acc[...] = jnp.zeros_like(acc)

        def body(w, c):
            cols = pl.ds(pl.multiple_of(w * 512, 512), 512)
            acc[...] += dot(xn[:, cols], g1[w].reshape(512, 640))
            return c

        lax.fori_loop(0, NZ, body, 0)

    lane_head = lax.div(iota((SEQ, 128), 1), KW)

    def by_head(x):
        return jnp.concatenate([jnp.where(lane_head == h, x, 0.0).astype(BF16) for h in range(HEADS)], axis=0)

    def prepare():
        gate = acc[:, 512:640] + bias[...]
        logs = (jnp.minimum(gate, 0.0) - jnp.log1p(jnp.exp(-jnp.abs(gate)))) / 16.0 + extra[...]
        hi = logs.astype(BF16)
        decay2[0:SEQ, :] = hi
        decay2[SEQ : 2 * SEQ, :] = (logs - hi.astype(F32)).astype(BF16)
        qf[...] = acc[:, 0:128].astype(BF16).astype(F32)
        kf[...] = acc[:, 128:256].astype(BF16).astype(F32)
        vals = acc[:, 256:512]
        lane_vhead = lax.div(iota((SEQ, 256), 1), VW)
        for h in range(HEADS):
            vbd[h * SEQ : (h + 1) * SEQ, :] = jnp.where(lane_vhead == h, vals, 0.0).astype(BF16)
        score[...] = 2.0 * dot_t(qf[...].astype(BF16), by_head(kf[...]))

    def level(l):
        left = (qf[...] * jnp.exp(dot(mats[2 * l], decay2[...]))).astype(BF16)
        right = by_head(kf[...] * jnp.exp(dot(mats[2 * l + 1], decay2[...])))
        differ = iota((SEQ, HEADS * SEQ), 0) ^ lax.rem(iota((SEQ, HEADS * SEQ), 1), SEQ)
        score[...] = jnp.where(differ >= 2 ** l, dot_t(left, right), score[...])

    def attend():
        mixed = dot(score[...].astype(BF16), vbd[...]) * (KW ** -0.5)
        sq = mixed * mixed
        sq_hi = sq.astype(BF16)
        sq_lo = (sq - sq_hi.astype(F32)).astype(BF16)
        ones = jnp.where(lax.div(iota((256, 256), 0), VW) == lax.div(iota((256, 256), 1), VW), 1.0, 0.0).astype(BF16)
        mean = (dot(sq_hi, ones) + dot(sq_lo, ones)) * (1.0 / VW)
        gains = jnp.concatenate([hgain[...]] * HEADS, axis=1)
        att[...] = (mixed * lax.rsqrt(mean + EPS) * gains).astype(BF16)

    def cols_of(c):
        return slice(c * D // CHUNKS, (c + 1) * D // CHUNKS)

    def copy_to(device, n, src, dst, sem):
        pltpu.make_async_remote_copy(
            src_ref=src, dst_ref=dst, send_sem=tsend.at[n], recv_sem=sem, device_id=device, device_id_type=MESH
        ).start()

    def slab_of(c):
        return lax.rem(z + SLAB_ORDER[c] + NZ, NZ)

    def project_out(n, c, left, weight, width):
        into, cols = parts[n], cols_of(c)
        rows = weight[c if n == 0 else slab_of(c)].reshape(D // NZ, width)
        into[:, :, :, cols] = dot_t(left[...], rows).astype(BF16).reshape(NTP // 2, 2, ROWS_OWN, D // NZ)
        copy_to(partner, n, into.at[:, 1 - core, :, cols], lands[n].at[:, :, cols], trecv.at[n, 0, c])

    def pair(n, c):
        cols = cols_of(c)
        both[n][:, :, cols] = (
            parts[n][:, core, :, cols].astype(F32) + lands[n][:, :, cols].astype(F32)
        ).astype(BF16)
        for k in (1, 2, 3):
            copy_to(peer(k), n, both[n].at[around(k), :, cols], gots[n].at[k - 1, :, cols], trecv.at[n, 1, c])

    def total(n, cols):
        s = parts[n][x, core, :, cols].astype(F32) + lands[n][x, :, cols].astype(F32)
        for k in range(3):
            s = s + gots[n][k, :, cols].astype(F32)
        return s

    own_rows = pl.ds(pl.multiple_of(t * ROWS_OWN, ROWS_OWN), ROWS_OWN)

    def residual_rows():
        r = (tok[own_rows, :].astype(F32) + total(0, slice(0, D))).astype(BF16).astype(F32)
        resid[...] = r
        n2[x, core] = (r * lax.rsqrt(jnp.mean(r * r, axis=-1, keepdims=True) + EPS) * gain2[...]).astype(BF16)
        for c in range(CHUNKS):
            mine = n2.at[x, core, :, cols_of(c)]
            for k in (1, 2, 3):
                copy_to(peer(k), 0, mine, mine, trecv.at[0, 2, c])
            copy_to(partner, 0, mine, mine, trecv.at[0, 3, c])

    def relay_normed(c):
        for k in (1, 2, 3):
            piece = n2.at[around(k), core, :, cols_of(c)]
            copy_to(partner, 0, piece, piece, trecv.at[0, 3, c])

    def place_of(c):
        return pl.ds(pl.multiple_of(slab_of(c) * (D // NZ), D // NZ), D // NZ)

    def out_at(i, c):
        rows = pl.ds(pl.multiple_of((2 * i + core) * ROWS_OWN, ROWS_OWN), ROWS_OWN)
        return out.at[rows, place_of(c)]

    def put(i, c):
        piece = fin.at[i, :, cols_of(c)]
        copy_to(partner, 1, piece, out_at(i, c), trecv.at[1, 3, c])
        pltpu.make_async_copy(piece, out_at(i, c), lsem.at[5]).start()

    def layer_out(c):
        cols, at = cols_of(c), place_of(c)
        fin[x, :, cols] = (resid[:, at] + total(1, cols)).astype(BF16)
        for k in (1, 2, 3):
            copy_to(peer(k), 1, fin.at[x, :, cols], fin.at[x, :, cols], trecv.at[1, 2, c])
        put(x, c)

    def relay_out(c):
        for k in (1, 2, 3):
            put(around(k), c)

    def end():
        wait_bytes(fin, lsem.at[5])

    def take_exchange(what):
        n, c = int(what[1]), int(what[2])
        kind = "dxsf".index(what[0])
        ref = lands[n].at[:, :, cols_of(c)] if what[0] in "df" else gots[n].at[:, :, cols_of(c)]
        wait_bytes(ref, trecv.at[n, kind, c])

    def gate_up():
        acc2[...] = jnp.zeros_like(acc2)

        def body(w, c):
            cols = pl.ds(pl.multiple_of(w * 512, 512), 512)
            acc2[...] += dot(n2[:, :, :, cols].reshape(SEQ, 512), g3[w].reshape(512, 768))
            return c

        lax.fori_loop(0, NZ, body, 0)

    def hidden():
        gated = acc2[:, 0:384]
        hid[...] = (gated / (1.0 + jnp.exp(-gated)) * acc2[:, 384:768]).astype(BF16)

    work = dict(
        norm=norm, mats=build, project=project, prepare=prepare, attend=attend,
        residual=residual_rows, gate_up=gate_up, hidden=hidden, end=end,
        **{f"level{l}": functools.partial(level, l) for l in range(LEVELS)},
        **{f"pair{n}{c}": functools.partial(pair, n, c) for n in (0, 1) for c in range(CHUNKS)},
    )
    for c in range(CHUNKS):
        work[f"mix{c}"] = functools.partial(project_out, 0, c, att, g2, 256)
        work[f"down{c}"] = functools.partial(project_out, 1, c, hid, g4, 384)
        work[f"relay0{c}"] = functools.partial(relay_normed, c)
        work[f"relay1{c}"] = functools.partial(relay_out, c)
        work[f"layer{c}"] = functools.partial(layer_out, c)
    waiting = set(range(4))
    for verb, what in link_plan(NEAR):
        with jax.named_scope(f"{verb}_{what}".replace(" ", "")):
            if verb == "work":
                work[what]()
            elif verb == "send":
                if what[0] in waiting:
                    waiting.discard(what[0])
                    own[what[0]].wait()
                send_weight(*what)
            elif isinstance(what, str):
                take_exchange(what)
            else:
                take_weight(*what)
    for g in range(4):
        wait_bytes(bufs[g].at[0:3], send.at[g])
        wait_bytes(bufs[g].at[3, 0:7], send.at[g])
    for n in (0, 1):
        wait_bytes(parts[n], tsend.at[n])
        wait_bytes(parts[n].at[0:3], tsend.at[n])


def shards(
    tokens, attention_norm_gain, query_weight, key_weight, value_weight, decay_weight, decay_gate_bias,
    decay_spike_extra, head_output_gain, output_weight, channel_norm_gain, gate_weight, up_weight, down_weight,
):
    hbm = pl.BlockSpec(memory_space=pltpu.HBM)
    widths = [sum(p) for p in PARTS]
    return pl.pallas_call(
        layer_kernel,
        out_shape=jax.ShapeDtypeStruct((SEQ, D), BF16),
        in_specs=[hbm] * 14,
        out_specs=pl.BlockSpec(memory_space=pl.ANY),
        scratch_shapes=[
            pltpu.VMEM((SEQ, D), BF16),
            pltpu.VMEM((1, D), F32),
            pltpu.VMEM((1, 128), F32),
            pltpu.VMEM((HEADS, SEQ), F32),
            pltpu.VMEM((1, VW), F32),
            pltpu.VMEM((1, D), F32),
            pltpu.VMEM((SEQ, 128), F32),
            pltpu.VMEM((NTP // 2, ROWS_OWN, D), BF16),
            *(pltpu.VMEM((NZ, NY, SLAB, w), BF16) for w in widths),
            pltpu.VMEM((SEQ, D), BF16),
            pltpu.VMEM((SEQ, 640), F32),
            pltpu.VMEM((2 * LEVELS, SEQ, 2 * SEQ), BF16),
            pltpu.VMEM((SEQ, HEADS * SEQ), F32),
            pltpu.VMEM((SEQ, 256), BF16),
            pltpu.VMEM((NTP // 2, 2, ROWS_OWN, D), BF16),
            pltpu.VMEM((SEQ, 768), F32),
            pltpu.VMEM((SEQ, 384), BF16),
            pltpu.VMEM((ROWS_OWN, D), F32),
            pltpu.VMEM((2 * SEQ, 128), BF16),
            pltpu.VMEM((SEQ, 128), F32),
            pltpu.VMEM((SEQ, 128), F32),
            pltpu.VMEM((HEADS * SEQ, 256), BF16),
            *[pltpu.VMEM((NTP // 2, 2, ROWS_OWN, D), BF16)] * 2,
            *[pltpu.VMEM((NTP // 2, ROWS_OWN, D), BF16)] * 4,
            *[pltpu.VMEM((NTP // 2 - 1, ROWS_OWN, D), BF16)] * 2,
            pltpu.SemaphoreType.DMA((12,)),
            pltpu.SemaphoreType.DMA((4,)),
            pltpu.SemaphoreType.DMA((4, len(TAKES))),
            pltpu.SemaphoreType.DMA((2,)),
            pltpu.SemaphoreType.DMA((2, 4, CHUNKS)),
        ],
        compiler_params=pltpu.CompilerParams(collective_id=0, has_side_effects=True),
    )(
        tokens,
        attention_norm_gain.reshape(1, D),
        decay_gate_bias.reshape(1, 128),
        decay_spike_extra.T,
        head_output_gain.reshape(1, VW),
        channel_norm_gain.reshape(1, D),
        query_weight, key_weight, value_weight, decay_weight, output_weight, gate_weight, up_weight, down_weight,
    )


def solution(mesh):
    rows, w = P(("rep", "fs"), None), P("fs", "tp")
    in_specs = (rows, P(), w, w, w, w, P("tp"), P(("rep", "fs"), "tp"), P(), w, P(), w, w, w)
    return jax.shard_map(shards, mesh=mesh, in_specs=in_specs, out_specs=rows, check_vma=False)
```

```python
import functools

import jax
import jax.numpy as jnp
from jax import lax
from jax.experimental import pallas as pl
from jax.experimental.pallas import tpu as pltpu
from jax.sharding import PartitionSpec as P

MESH = pl.DeviceIdType.MESH
F32, BF16 = jnp.float32, jnp.bfloat16
NY, NZ, NTP = 8, 4, 8
SEQ, D = 128, 2048
SLAB = D // (NY * NZ)
HEADS, KW, VW = 4, 32, 64
LEVELS = 7
EPS = 1e-6
PARTS = ((128, 128, 256, 128), (256,), (384, 384), (384,))
A_ROWS = (32, 48, 32, 64)
ROWS_OWN = SEQ // NTP
CHUNKS = NZ
SLAB_ORDER = (0, -1, 1, 2)


def messages(g):
    ra = A_ROWS[g]
    rows_a, rows_b = slice(0, ra), slice(ra, SLAB)
    half_a = (slice(0, 16 * ((ra // 16 + 1) // 2)), slice(16 * ((ra // 16 + 1) // 2), ra))
    half_b = (slice(ra, ra + 16 * ((SLAB - ra) // 32)), slice(ra + 16 * ((SLAB - ra) // 32), SLAB))
    out = {}
    for d in (0, 1):
        back = -1 if d == 0 else 1
        for s in range(4):
            out["ay", d, s] = ("y", 0, back * s, rows_a if s < 3 else half_a[d], (("ay", s - 1),) if s else (), ("ay", s))
        for i, off in enumerate((0, -1, 1, -2, 2, -3, 3, 4)):
            out["az", d, i] = ("z", 0, off, rows_a, (("ay", (i - 1) // 2),) if i else (), ("az", 0))
        out["az", d, 8] = ("z", back, slice(4 * d, 4 * d + 4), rows_a, (("az", 0),), ("az", 1))
        out["bz", d, 0] = ("z", 0, 0, rows_b, (), ("bz", 0))
        if half_b[d].stop > half_b[d].start:
            out["bz", d, 1] = ("z", back, 0, half_b[d], (("bz", 0),), ("bz", 1))
        for i, off in enumerate((0, -1, 1, 2)):
            out["by", d, i] = ("y", off, 0, rows_b, (("bz", i // 3),) if i else (), ("by", 0))
        for s in (1, 2):
            for h in (0, 1):
                half = slice(2 * h, 2 * h + 2)
                out["by", d, 2 + 2 * s + h] = (
                    "y", half, back * s, rows_b, (("by", 2 * s - 3 + h if s > 1 else 0),), ("by", 2 * s - 1 + h),
                )
        out["by", d, 8] = ("y", slice(2 * d, 2 * d + 2), back * 3, rows_b, (("by", 3 + d),), ("by", 5))
    return {m: v for m, v in out.items() if extent(v[3])}


TAKES = [("ay", 0), ("ay", 1), ("ay", 2), ("ay", 3), ("az", 0), ("az", 1), ("bz", 0), ("bz", 1), *(("by", i) for i in range(6))]


def extent(i):
    return i.stop - i.start if isinstance(i, slice) else 1


def link_plan(near, hop=2.4, rate=46.6e3, times=None):
    table = {(g, *m): v for g in range(4) for m, v in messages(g).items()}
    need = {m: {(m[0], *x) for x in v[4]} for m, v in table.items()}
    feeds, then = {}, {}
    for m, v in table.items():
        feeds.setdefault((m[0], *v[5]), set()).add(m)
        for x in need[m]:
            then.setdefault(x, []).append(m)

    def urgency(m):
        g, name, d, i = m
        second = name == "by" or name == "az"
        return (BASE[g] if second else LIGHT[g], i, d)

    ready = {(a, d): [] for a in ("y", "z") for d in (0, 1)}
    free = dict.fromkeys(ready, 0.0)
    left = [sum(x[0] == g for x in feeds) for g in range(4)]
    for m, v in table.items():
        if not need[m]:
            ready[v[0], m[2]].append(m)
    now, ops, have, coming, todo = 0.2, [], set(), [], list(WORK)
    landed = {}
    def fill(until):
        nonlocal now
        before = len(ops)
        for l, queue in ready.items():
            while queue and free[l] < until:
                m = min(queue, key=urgency)
                queue.remove(m)
                v = table[m]
                size = extent(v[1]) * extent(v[2]) * extent(v[3]) * sum(PARTS[m[0]]) * 2
                free[l] = max(now, free[l]) + size / rate
                landed[m] = free[l] + hop
                take = (m[0], *v[5])
                if all(x in landed for x in feeds[take]):
                    coming.append((max(landed[x] for x in feeds[take]), len(ops), take))
                ops.append(("send", m))
                now += 0.02
        return len(ops) > before

    while todo or coming:
        fill(now + near)
        coming.sort()
        if coming and coming[0][0] <= now:
            m = coming.pop(0)[2]
            ops.append(("take", m))
            now += 0.02
            have.add(m)
            if isinstance(m, str):
                continue
            left[m[0]] -= 1
            if left[m[0]] == 0:
                have.add(m[0])
                if times is not None:
                    times[m[0]] = now
            for x in then.get(m, ()):
                need[x].discard(m)
                if not need[x]:
                    ready[table[x][0], x[2]].append(x)
            continue
        item = next((w for w in todo if all(q in have for q in w[2])), None)
        if item:
            todo.remove(item)
            name, span, _, gives = item
            have.add(name)
            fill(now + span)
            now += span
            ops.append(("work", name))
            coming.extend((now + TURN[x[0]], len(ops), x) for x in gives)
        elif not fill(min(coming)[0] if coming else now + 1e3):
            now = max(now, min(coming)[0])
    if times is not None:
        times["end"] = now
    return ops


EACH = range(CHUNKS)
LAST = ((3, "ay", 0), (3, "ay", 1), (3, "ay", 2), (3, "ay", 3)), ((3, "az", 0),), ((3, "az", 0),), ((3, "az", 1),)
WORK = (
    ("norm", 0.92, (), ()),
    ("mats", 0.67, (), ()),
    ("project", 1.1, ("norm", 0), ()),
    ("prepare", 0.27, ("project", "mats"), ()),
    ("levels0", 1.2, ("prepare",), ()),
    ("levels1", 0.9, ("levels0",), ()),
    ("attend", 0.36, ("levels1",), ()),
    *((f"mix{c}", 0.23, ("attend", 1), (f"d0{c}",)) for c in EACH),
    *((f"pair0{c}", 0.05, (f"d0{c}",), (f"x0{c}",)) for c in EACH),
    *((f"residual{c}", 0.08, (f"x0{c}", *((f"residual{c - 1}",) if c else ())), (f"s0{c}",)) for c in EACH),
    *((f"relay0{c}", 0.03, (f"s0{c}",), (f"f0{c}",)) for c in EACH),
    ("gate_up", 1.12, (*(f"f0{c}" for c in EACH), *(f"relay0{c}" for c in EACH), 2), ()),
    ("hidden", 0.07, ("gate_up",), ()),
    *((f"down{c}", 0.27, ("hidden", *LAST[c]), (f"d1{c}",)) for c in EACH),
    *((f"pair1{c}", 0.05, (f"d1{c}",), (f"x1{c}",)) for c in EACH),
    *((f"layer{c}", 0.05, (f"x1{c}",), (f"s1{c}",)) for c in EACH),
    *((f"relay1{c}", 0.03, (f"s1{c}",), (f"f1{c}",)) for c in EACH),
    ("end", 0.1, (*(f"f1{c}" for c in EACH), *(f"relay1{c}" for c in EACH)), ()),
)
TURN = dict(d=1.3, x=4.9, s=4.4, f=1.3)
NEAR = 0.3
BASE, LIGHT = (0, -1, 20, 22), (-12, -13, 2, 19)


def dot(a, b):
    return jnp.dot(a, b, preferred_element_type=F32)


def dot_t(a, b):
    return lax.dot_general(a, b, (((1,), (1,)), ((), ())), preferred_element_type=F32)


def iota(shape, axis):
    return lax.broadcasted_iota(jnp.int32, shape, axis)


def layer_kernel(
    tok_hbm, gain1_hbm, bias_hbm, spike_hbm, hgain_hbm, gain2_hbm, wq, wk, wv, wd, wo, wg, wu, wdn,
    out,
    tok, gain1, bias, spike, hgain, gain2, extra, fin,
    g1, g2, g3, g4, xn, acc, mats, score, att, n2, acc2, hid, resid, decay2, qf, kf, vbd,
    part, part2, land, land2, both1, both2, got, got2, factors,
    lsem, send, recv, tsend, trecv,
):
    bufs = (g1, g2, g3, g4)
    parts, lands, both, gots = (part, part2), (land, land2), (both1, both2), (got, got2)
    rep, f, t = lax.axis_index("rep"), lax.axis_index("fs"), lax.axis_index("tp")
    y, z = lax.rem(f, NY), lax.div(f, NY)
    zz = rep * NZ + z

    def at_y(k):
        return (rep, z * NY + lax.rem(y + k + NY, NY), t)

    def at_z(k):
        w = lax.rem(zz + k + 2 * NZ, 2 * NZ)
        return (lax.div(w, NZ), lax.rem(w, NZ) * NY + y, t)

    ynb, znb = (at_y(1), at_y(-1)), (at_z(1), at_z(-1))

    x, core = lax.div(t, 2), lax.rem(t, 2)
    partner = (rep, f, t + 1 - 2 * core)

    def around(k):
        return lax.rem(x + k, NTP // 2)

    def peer(k):
        return (rep, f, 2 * around(k) + core)

    barrier = pltpu.get_barrier_semaphore()
    others = [*ynb, *znb, partner, *(peer(k) for k in (1, 2, 3))]
    for d in others:
        pl.semaphore_signal(barrier, inc=1, device_id=d, device_id_type=MESH)

    own = []
    srcs = ((wq, wk, wv, wd), (wo,), (wg, wu), (wdn,))
    for g in range(4):
        at, copies = 0, []
        for src, width in zip(srcs[g], PARTS[g]):
            copies.append(pltpu.make_async_copy(src, bufs[g].at[z, y, :, at : at + width], lsem.at[g]))
            at += width
        for c in copies:
            c.start()
        own.append(pltpu.make_async_copy(bufs[g].at[z, y], bufs[g].at[z, y], lsem.at[g]))
        if g == 0:
            small = ((gain1_hbm, gain1), (bias_hbm, bias), (spike_hbm, spike), (hgain_hbm, hgain), (gain2_hbm, gain2))
            fetches = [
                pltpu.make_async_copy(src, dst, lsem.at[6 + i]) for i, (src, dst) in enumerate(((tok_hbm, tok), *small))
            ]
            for c in fetches:
                c.start()

    pl.semaphore_wait(barrier, len(others))

    tables = [messages(g) for g in range(4)]

    def place(i, at, n):
        return i if isinstance(i, slice) else lax.rem(at + i + n, n)

    def send_weight(g, name, d, i):
        ring, zs, ys, rows, _, take = tables[g][name, d, i]
        ref = bufs[g].at[place(zs, z, NZ), place(ys, y, NY), rows, :]
        pltpu.make_async_remote_copy(
            src_ref=ref, dst_ref=ref, send_sem=send.at[g], recv_sem=recv.at[g, TAKES.index(take)],
            device_id=(ynb if ring == "y" else znb)[d], device_id_type=MESH,
        ).start()

    def wait_bytes(ref, sem):
        pltpu.make_async_copy(ref, ref, sem).wait()

    def take_weight(g, name, i):
        slabs, rows = 0, None
        for v in tables[g].values():
            if v[5] == (name, i):
                whole = extent(v[3])
                slabs += extent(v[1]) * extent(v[2]) * whole
        for nz, ny, size in ((1, 1, SLAB), (1, 2, SLAB), (1, 4, SLAB), (1, 8, SLAB), (2, 8, SLAB), (3, 8, SLAB)):
            if slabs % (nz * ny * 16) == 0 and slabs <= nz * ny * size:
                ref = bufs[g].at[0:nz, 0:ny, 0 : slabs // (nz * ny), :]
                wait_bytes(ref, recv.at[g, TAKES.index((name, i))])
                return
        raise ValueError(name)

    def norm_rows(i, c):
        r = pl.ds(pl.multiple_of(i * 16, 16), 16)
        v = tok[r, :].astype(F32)
        xn[r, :] = (v * lax.rsqrt(jnp.mean(v * v, axis=-1, keepdims=True) + EPS) * gain1[...]).astype(BF16)
        return c

    def norm():
        for c in fetches:
            c.wait()
        lax.fori_loop(0, SEQ // 16, norm_rows, 0)

    def build_mats(l, c):
        ti, si = iota((SEQ, 2 * SEQ), 0), lax.rem(iota((SEQ, 2 * SEQ), 1), SEQ)
        same = lax.shift_right_logical(ti, l) == lax.shift_right_logical(si, l)
        back = (ti - si) * (2 * (lax.shift_right_logical(ti, l) & 1) - 1)
        mats[2 * l] = jnp.where(same & (back >= 0), 1.0, 0.0).astype(BF16)
        mats[2 * l + 1] = jnp.where(same & (back > 0), 1.0, 0.0).astype(BF16)
        return c

    def build():
        lax.fori_loop(0, LEVELS, build_mats, 0)
        heads = jnp.where(lax.div(iota((HEADS, 128), 1), KW) == iota((HEADS, 128), 0), 1.0, 0.0)
        extra[...] = lax.dot_general(
            spike[...], heads, (((0,), (0,)), ((), ())), precision=lax.Precision.HIGHEST, preferred_element_type=F32
        )

    def project():
        acc[...] = jnp.zeros_like(acc)

        def body(w, c):
            cols = pl.ds(pl.multiple_of(w * 512, 512), 512)
            acc[...] += dot(xn[:, cols], g1[w].reshape(512, 640))
            return c

        lax.fori_loop(0, NZ, body, 0)

    lane_head = lax.div(iota((SEQ, 128), 1), KW)

    def by_head(x):
        return jnp.concatenate([jnp.where(lane_head == h, x, 0.0).astype(BF16) for h in range(HEADS)], axis=0)

    def prepare():
        gate = acc[:, 512:640] + bias[...]
        logs = (jnp.minimum(gate, 0.0) - jnp.log1p(jnp.exp(-jnp.abs(gate)))) / 16.0 + extra[...]
        hi = logs.astype(BF16)
        decay2[0:SEQ, :] = hi
        decay2[SEQ : 2 * SEQ, :] = (logs - hi.astype(F32)).astype(BF16)
        qf[...] = acc[:, 0:128].astype(BF16).astype(F32)
        kf[...] = acc[:, 128:256].astype(BF16).astype(F32)
        vals = acc[:, 256:512]
        lane_vhead = lax.div(iota((SEQ, 256), 1), VW)
        for h in range(HEADS):
            vbd[h * SEQ : (h + 1) * SEQ, :] = jnp.where(lane_vhead == h, vals, 0.0).astype(BF16)
        score[...] = 2.0 * dot_t(qf[...].astype(BF16), by_head(kf[...]))

    def level(l):
        left = (qf[...] * jnp.exp(dot(mats[2 * l], decay2[...]))).astype(BF16)
        right = by_head(kf[...] * jnp.exp(dot(mats[2 * l + 1], decay2[...])))
        differ = iota((SEQ, HEADS * SEQ), 0) ^ lax.rem(iota((SEQ, HEADS * SEQ), 1), SEQ)
        score[...] = jnp.where(differ >= 2 ** l, dot_t(left, right), score[...])

    def attend():
        mixed = dot(score[...].astype(BF16), vbd[...]) * (KW ** -0.5)
        sq = mixed * mixed
        sq_hi = sq.astype(BF16)
        sq_lo = (sq - sq_hi.astype(F32)).astype(BF16)
        ones = jnp.where(lax.div(iota((256, 256), 0), VW) == lax.div(iota((256, 256), 1), VW), 1.0, 0.0).astype(BF16)
        mean = (dot(sq_hi, ones) + dot(sq_lo, ones)) * (1.0 / VW)
        gains = jnp.concatenate([hgain[...]] * HEADS, axis=1)
        att[...] = (mixed * lax.rsqrt(mean + EPS) * gains).astype(BF16)

    def cols_of(c):
        return slice(c * D // CHUNKS, (c + 1) * D // CHUNKS)

    def copy_to(device, n, src, dst, sem):
        pltpu.make_async_remote_copy(
            src_ref=src, dst_ref=dst, send_sem=tsend.at[n], recv_sem=sem, device_id=device, device_id_type=MESH
        ).start()

    def slab_of(c):
        return lax.rem(z + SLAB_ORDER[c] + NZ, NZ)

    def project_out(n, c, left, weight, width):
        into, cols = parts[n], cols_of(c)
        rows = weight[c if n == 0 else slab_of(c)].reshape(D // NZ, width)
        into[:, :, :, cols] = dot_t(left[...], rows).astype(BF16).reshape(NTP // 2, 2, ROWS_OWN, D // NZ)
        copy_to(partner, n, into.at[:, 1 - core, :, cols], lands[n].at[:, :, cols], trecv.at[n, 0, c])

    def pair(n, c):
        cols = cols_of(c)
        both[n][:, :, cols] = (
            parts[n][:, core, :, cols].astype(F32) + lands[n][:, :, cols].astype(F32)
        ).astype(BF16)
        for k in (1, 2, 3):
            copy_to(peer(k), n, both[n].at[around(k), :, cols], gots[n].at[k - 1, :, cols], trecv.at[n, 1, c])

    def total(n, cols):
        s = parts[n][x, core, :, cols].astype(F32) + lands[n][x, :, cols].astype(F32)
        for k in range(3):
            s = s + gots[n][k, :, cols].astype(F32)
        return s

    own_rows = pl.ds(pl.multiple_of(t * ROWS_OWN, ROWS_OWN), ROWS_OWN)

    def residual(c):
        cols = cols_of(c)
        r = (tok[own_rows, cols].astype(F32) + total(0, cols)).astype(BF16).astype(F32)
        resid[:, cols] = r
        mine = n2.at[x, core, :, cols]
        mine[...] = (r * gain2[:, cols]).astype(BF16)
        pieces = [mine]
        if c == CHUNKS - 1:
            r = resid[...]
            factor = lax.rsqrt(jnp.mean(r * r, axis=-1, keepdims=True) + EPS)
            factors[x, core] = jnp.broadcast_to(factor, (ROWS_OWN, 128))
            pieces.append(factors.at[x, core])
        for piece in pieces:
            for k in (1, 2, 3):
                copy_to(peer(k), 0, piece, piece, trecv.at[0, 2, c])
            copy_to(partner, 0, piece, piece, trecv.at[0, 3, c])

    def relay_normed(c):
        for k in (1, 2, 3):
            piece = n2.at[around(k), core, :, cols_of(c)]
            copy_to(partner, 0, piece, piece, trecv.at[0, 3, c])
            if c == CHUNKS - 1:
                piece = factors.at[around(k), core]
                copy_to(partner, 0, piece, piece, trecv.at[0, 3, c])

    def place_of(c):
        return pl.ds(pl.multiple_of(slab_of(c) * (D // NZ), D // NZ), D // NZ)

    def out_at(i, c):
        rows = pl.ds(pl.multiple_of((2 * i + core) * ROWS_OWN, ROWS_OWN), ROWS_OWN)
        return out.at[rows, place_of(c)]

    def put(i, c):
        piece = fin.at[i, :, cols_of(c)]
        copy_to(partner, 1, piece, out_at(i, c), trecv.at[1, 3, c])
        pltpu.make_async_copy(piece, out_at(i, c), lsem.at[5]).start()

    def layer_out(c):
        cols, at = cols_of(c), place_of(c)
        fin[x, :, cols] = (resid[:, at] + total(1, cols)).astype(BF16)
        for k in (1, 2, 3):
            copy_to(peer(k), 1, fin.at[x, :, cols], fin.at[x, :, cols], trecv.at[1, 2, c])
        put(x, c)

    def relay_out(c):
        for k in (1, 2, 3):
            put(around(k), c)

    def end():
        wait_bytes(fin, lsem.at[5])

    def take_exchange(what):
        n, c = int(what[1]), int(what[2])
        kind = "dxsf".index(what[0])
        wide = D // CHUNKS + (256 if n == 0 and what[0] in "sf" and c == CHUNKS - 1 else 0)
        ref = (lands if what[0] in "df" else gots)[n].at[:, :, 0:wide]
        wait_bytes(ref, trecv.at[n, kind, c])

    def gate_up():
        acc2[...] = jnp.zeros_like(acc2)

        def body(w, c):
            cols = pl.ds(pl.multiple_of(w * 512, 512), 512)
            acc2[...] += dot(n2[:, :, :, cols].reshape(SEQ, 512), g3[w].reshape(512, 768))
            return c

        lax.fori_loop(0, NZ, body, 0)

    def hidden():
        factor = factors[...].reshape(SEQ, 128)[:, 0:1]
        gated = acc2[:, 0:384] * factor
        hid[...] = (gated / (1.0 + jnp.exp(-gated)) * (acc2[:, 384:768] * factor)).astype(BF16)

    work = dict(
        norm=norm, mats=build, project=project, prepare=prepare, attend=attend,
        gate_up=gate_up, hidden=hidden, end=end,
        levels0=lambda: [level(l) for l in range(4)], levels1=lambda: [level(l) for l in range(4, LEVELS)],
        **{f"pair{n}{c}": functools.partial(pair, n, c) for n in (0, 1) for c in range(CHUNKS)},
    )
    for c in range(CHUNKS):
        work[f"mix{c}"] = functools.partial(project_out, 0, c, att, g2, 256)
        work[f"down{c}"] = functools.partial(project_out, 1, c, hid, g4, 384)
        work[f"residual{c}"] = functools.partial(residual, c)
        work[f"relay0{c}"] = functools.partial(relay_normed, c)
        work[f"relay1{c}"] = functools.partial(relay_out, c)
        work[f"layer{c}"] = functools.partial(layer_out, c)
    waiting = set(range(4))
    for verb, what in link_plan(NEAR):
        with jax.named_scope(f"{verb}_{what}".replace(" ", "")):
            if verb == "work":
                work[what]()
            elif verb == "send":
                if what[0] in waiting:
                    waiting.discard(what[0])
                    own[what[0]].wait()
                send_weight(*what)
            elif isinstance(what, str):
                take_exchange(what)
            else:
                take_weight(*what)
    for g in range(4):
        wait_bytes(bufs[g].at[0:3], send.at[g])
        wait_bytes(bufs[g].at[3, 0:7], send.at[g])
    for n in (0, 1):
        wait_bytes(parts[n], tsend.at[n])
        wait_bytes(parts[n].at[0:3], tsend.at[n])
    wait_bytes(factors.at[0:3], tsend.at[0])
    wait_bytes(factors.at[3, 0], tsend.at[0])


def shards(
    tokens, attention_norm_gain, query_weight, key_weight, value_weight, decay_weight, decay_gate_bias,
    decay_spike_extra, head_output_gain, output_weight, channel_norm_gain, gate_weight, up_weight, down_weight,
):
    hbm = pl.BlockSpec(memory_space=pltpu.HBM)
    widths = [sum(p) for p in PARTS]
    return pl.pallas_call(
        layer_kernel,
        out_shape=jax.ShapeDtypeStruct((SEQ, D), BF16),
        in_specs=[hbm] * 14,
        out_specs=pl.BlockSpec(memory_space=pl.ANY),
        scratch_shapes=[
            pltpu.VMEM((SEQ, D), BF16),
            pltpu.VMEM((1, D), F32),
            pltpu.VMEM((1, 128), F32),
            pltpu.VMEM((HEADS, SEQ), F32),
            pltpu.VMEM((1, VW), F32),
            pltpu.VMEM((1, D), F32),
            pltpu.VMEM((SEQ, 128), F32),
            pltpu.VMEM((NTP // 2, ROWS_OWN, D), BF16),
            *(pltpu.VMEM((NZ, NY, SLAB, w), BF16) for w in widths),
            pltpu.VMEM((SEQ, D), BF16),
            pltpu.VMEM((SEQ, 640), F32),
            pltpu.VMEM((2 * LEVELS, SEQ, 2 * SEQ), BF16),
            pltpu.VMEM((SEQ, HEADS * SEQ), F32),
            pltpu.VMEM((SEQ, 256), BF16),
            pltpu.VMEM((NTP // 2, 2, ROWS_OWN, D), BF16),
            pltpu.VMEM((SEQ, 768), F32),
            pltpu.VMEM((SEQ, 384), BF16),
            pltpu.VMEM((ROWS_OWN, D), F32),
            pltpu.VMEM((2 * SEQ, 128), BF16),
            pltpu.VMEM((SEQ, 128), F32),
            pltpu.VMEM((SEQ, 128), F32),
            pltpu.VMEM((HEADS * SEQ, 256), BF16),
            *[pltpu.VMEM((NTP // 2, 2, ROWS_OWN, D), BF16)] * 2,
            *[pltpu.VMEM((NTP // 2, ROWS_OWN, D), BF16)] * 4,
            *[pltpu.VMEM((NTP // 2 - 1, ROWS_OWN, D), BF16)] * 2,
            pltpu.VMEM((NTP // 2, 2, ROWS_OWN, 128), F32),
            pltpu.SemaphoreType.DMA((12,)),
            pltpu.SemaphoreType.DMA((4,)),
            pltpu.SemaphoreType.DMA((4, len(TAKES))),
            pltpu.SemaphoreType.DMA((2,)),
            pltpu.SemaphoreType.DMA((2, 4, CHUNKS)),
        ],
        compiler_params=pltpu.CompilerParams(collective_id=0, has_side_effects=True),
    )(
        tokens,
        attention_norm_gain.reshape(1, D),
        decay_gate_bias.reshape(1, 128),
        decay_spike_extra.T,
        head_output_gain.reshape(1, VW),
        channel_norm_gain.reshape(1, D),
        query_weight, key_weight, value_weight, decay_weight, output_weight, gate_weight, up_weight, down_weight,
    )


def solution(mesh):
    rows, w = P(("rep", "fs"), None), P("fs", "tp")
    in_specs = (rows, P(), w, w, w, w, P("tp"), P(("rep", "fs"), "tp"), P(), w, P(), w, w, w)
    return jax.shard_map(shards, mesh=mesh, in_specs=in_specs, out_specs=rows, check_vma=False)
```

```python
import functools

import jax
import jax.numpy as jnp
from jax import lax
from jax.experimental import pallas as pl
from jax.experimental.pallas import tpu as pltpu
from jax.sharding import PartitionSpec as P

MESH = pl.DeviceIdType.MESH
F32, BF16 = jnp.float32, jnp.bfloat16
NY, NZ, NTP = 8, 4, 8
SEQ, D = 128, 2048
SLAB = D // (NY * NZ)
HEADS, KW, VW = 4, 32, 64
LEVELS = 7
EPS = 1e-6
PARTS = ((128, 128, 256, 128), (256,), (384, 384), (384,))
A_ROWS = (32, 48, 32, 64)
ROWS_OWN = SEQ // NTP
CHUNKS = NZ
SLAB_ORDER = (0, -1, 1, 2)


def messages(g):
    ra = A_ROWS[g]
    rows_a, rows_b = slice(0, ra), slice(ra, SLAB)
    half_a = (slice(0, 16 * ((ra // 16 + 1) // 2)), slice(16 * ((ra // 16 + 1) // 2), ra))
    half_b = (slice(ra, ra + 16 * ((SLAB - ra) // 32)), slice(ra + 16 * ((SLAB - ra) // 32), SLAB))
    out = {}
    for d in (0, 1):
        back = -1 if d == 0 else 1
        for s in range(4):
            out["ay", d, s] = ("y", 0, back * s, rows_a if s < 3 else half_a[d], (("ay", s - 1),) if s else (), ("ay", s))
        for i, off in enumerate((0, -1, 1, -2, 2, -3, 3, 4)):
            out["az", d, i] = ("z", 0, off, rows_a, (("ay", (i - 1) // 2),) if i else (), ("az", 0))
        out["az", d, 8] = ("z", back, slice(4 * d, 4 * d + 4), rows_a, (("az", 0),), ("az", 1))
        out["bz", d, 0] = ("z", 0, 0, rows_b, (), ("bz", 0))
        if half_b[d].stop > half_b[d].start:
            out["bz", d, 1] = ("z", back, 0, half_b[d], (("bz", 0),), ("bz", 1))
        for i, off in enumerate((0, -1, 1, 2)):
            out["by", d, i] = ("y", off, 0, rows_b, (("bz", i // 3),) if i else (), ("by", 0))
        for s in (1, 2):
            for h in (0, 1):
                half = slice(2 * h, 2 * h + 2)
                out["by", d, 2 + 2 * s + h] = (
                    "y", half, back * s, rows_b, (("by", 2 * s - 3 + h if s > 1 else 0),), ("by", 2 * s - 1 + h),
                )
        out["by", d, 8] = ("y", slice(2 * d, 2 * d + 2), back * 3, rows_b, (("by", 3 + d),), ("by", 5))
    return {m: v for m, v in out.items() if extent(v[3])}


TAKES = [("ay", 0), ("ay", 1), ("ay", 2), ("ay", 3), ("az", 0), ("az", 1), ("bz", 0), ("bz", 1), *(("by", i) for i in range(6))]


def extent(i):
    return i.stop - i.start if isinstance(i, slice) else 1


def link_plan(near, hop=2.4, rate=46.6e3, times=None):
    table = {(g, *m): v for g in range(4) for m, v in messages(g).items()}
    need = {m: {(m[0], *x) for x in v[4]} for m, v in table.items()}
    feeds, then = {}, {}
    for m, v in table.items():
        feeds.setdefault((m[0], *v[5]), set()).add(m)
        for x in need[m]:
            then.setdefault(x, []).append(m)

    def urgency(m):
        g, name, d, i = m
        second = name == "by" or name == "az"
        return (BASE[g] if second else LIGHT[g], i, d)

    ready = {(a, d): [] for a in ("y", "z") for d in (0, 1)}
    free = dict.fromkeys(ready, 0.0)
    left = [sum(x[0] == g for x in feeds) for g in range(4)]
    for m, v in table.items():
        if not need[m]:
            ready[v[0], m[2]].append(m)
    now, ops, have, coming, todo = 0.2, [], set(), [], list(WORK)
    landed = {}
    def fill(until):
        nonlocal now
        before = len(ops)
        for l, queue in ready.items():
            while queue and free[l] < until:
                m = min(queue, key=urgency)
                queue.remove(m)
                v = table[m]
                size = extent(v[1]) * extent(v[2]) * extent(v[3]) * sum(PARTS[m[0]]) * 2
                free[l] = max(now, free[l]) + size / rate
                landed[m] = free[l] + hop
                take = (m[0], *v[5])
                if all(x in landed for x in feeds[take]):
                    coming.append((max(landed[x] for x in feeds[take]), len(ops), take))
                ops.append(("send", m))
                now += 0.02
        return len(ops) > before

    while todo or coming:
        fill(now + near)
        coming.sort()
        if coming and coming[0][0] <= now:
            m = coming.pop(0)[2]
            ops.append(("take", m))
            now += 0.02
            have.add(m)
            if isinstance(m, str):
                continue
            left[m[0]] -= 1
            if left[m[0]] == 0:
                have.add(m[0])
                if times is not None:
                    times[m[0]] = now
            for x in then.get(m, ()):
                need[x].discard(m)
                if not need[x]:
                    ready[table[x][0], x[2]].append(x)
            continue
        item = next((w for w in todo if all(q in have for q in w[2])), None)
        if item:
            todo.remove(item)
            name, span, _, gives = item
            have.add(name)
            fill(now + span)
            now += span
            ops.append(("work", name))
            coming.extend((now + TURN[x[0]], len(ops), x) for x in gives)
        elif not fill(min(coming)[0] if coming else now + 1e3):
            now = max(now, min(coming)[0])
    if times is not None:
        times["end"] = now
    return ops


EACH = range(CHUNKS)
LAST = ((3, "ay", 0), (3, "ay", 1), (3, "ay", 2), (3, "ay", 3)), ((3, "az", 0),), ((3, "az", 0),), ((3, "az", 1),)
WORK = (
    ("norm", 0.92, (), ()),
    ("mats", 0.67, (), ()),
    ("project", 1.1, ("norm", 0), ()),
    ("prepare", 0.27, ("project", "mats"), ()),
    ("levels0", 1.2, ("prepare",), ()),
    ("levels1", 0.9, ("levels0",), ()),
    ("attend", 0.36, ("levels1",), ()),
    *((f"mix{c}", 0.23, ("attend", 1), (f"d0{c}",)) for c in EACH),
    *((f"pair0{c}", 0.05, (f"d0{c}",), (f"x0{c}",)) for c in EACH),
    *((f"residual{c}", 0.08, (f"x0{c}", *((f"residual{c - 1}",) if c else ())), (f"s0{c}",)) for c in EACH),
    *((f"relay0{c}", 0.03, (f"s0{c}",), ("f00",) if c == CHUNKS - 1 else ()) for c in EACH),
    ("gate_up", 1.12, ("f00", *(f"relay0{c}" for c in EACH), 2), ()),
    ("hidden", 0.07, ("gate_up",), ()),
    *((f"down{c}", 0.27, ("hidden", *LAST[c]), (f"d1{c}",)) for c in EACH),
    *((f"pair1{c}", 0.05, (f"d1{c}",), (f"x1{c}",)) for c in EACH),
    *((f"layer{c}", 0.05, (f"x1{c}",), (f"s1{c}",)) for c in EACH),
    *((f"relay1{c}", 0.03, (f"s1{c}",), ("f10",) if c == CHUNKS - 1 else ()) for c in EACH),
    ("end", 0.1, ("f10", *(f"relay1{c}" for c in EACH)), ()),
)
TURN = dict(d=1.3, x=4.9, s=4.4, f=1.3)
NEAR = 0.3
BASE, LIGHT = (0, -1, 20, 22), (-12, -13, 2, 19)


def dot(a, b):
    return jnp.dot(a, b, preferred_element_type=F32)


def dot_t(a, b):
    return lax.dot_general(a, b, (((1,), (1,)), ((), ())), preferred_element_type=F32)


def iota(shape, axis):
    return lax.broadcasted_iota(jnp.int32, shape, axis)


def layer_kernel(
    tok_hbm, gain1_hbm, bias_hbm, spike_hbm, hgain_hbm, gain2_hbm, wq, wk, wv, wd, wo, wg, wu, wdn,
    out,
    tok, gain1, bias, spike, hgain, gain2, extra, fin,
    g1, g2, g3, g4, xn, acc, mats, score, att, n2, acc2, hid, resid, decay2, qf, kf, vbd,
    part, part2, land, land2, both1, both2, got, got2, factors,
    lsem, send, recv, tsend, trecv,
):
    bufs = (g1, g2, g3, g4)
    parts, lands, both, gots = (part, part2), (land, land2), (both1, both2), (got, got2)
    rep, f, t = lax.axis_index("rep"), lax.axis_index("fs"), lax.axis_index("tp")
    y, z = lax.rem(f, NY), lax.div(f, NY)
    zz = rep * NZ + z

    def at_y(k):
        return (rep, z * NY + lax.rem(y + k + NY, NY), t)

    def at_z(k):
        w = lax.rem(zz + k + 2 * NZ, 2 * NZ)
        return (lax.div(w, NZ), lax.rem(w, NZ) * NY + y, t)

    ynb, znb = (at_y(1), at_y(-1)), (at_z(1), at_z(-1))

    x, core = lax.div(t, 2), lax.rem(t, 2)
    partner = (rep, f, t + 1 - 2 * core)

    def around(k):
        return lax.rem(x + k, NTP // 2)

    def peer(k):
        return (rep, f, 2 * around(k) + core)

    barrier = pltpu.get_barrier_semaphore()
    others = [*ynb, *znb, partner, *(peer(k) for k in (1, 2, 3))]
    for d in others:
        pl.semaphore_signal(barrier, inc=1, device_id=d, device_id_type=MESH)

    own = []
    srcs = ((wq, wk, wv, wd), (wo,), (wg, wu), (wdn,))
    for g in range(4):
        at, copies = 0, []
        for src, width in zip(srcs[g], PARTS[g]):
            copies.append(pltpu.make_async_copy(src, bufs[g].at[z, y, :, at : at + width], lsem.at[g]))
            at += width
        for c in copies:
            c.start()
        own.append(pltpu.make_async_copy(bufs[g].at[z, y], bufs[g].at[z, y], lsem.at[g]))
        if g == 0:
            small = ((gain1_hbm, gain1), (bias_hbm, bias), (spike_hbm, spike), (hgain_hbm, hgain), (gain2_hbm, gain2))
            fetches = [
                pltpu.make_async_copy(src, dst, lsem.at[6 + i]) for i, (src, dst) in enumerate(((tok_hbm, tok), *small))
            ]
            for c in fetches:
                c.start()

    pl.semaphore_wait(barrier, len(others))

    tables = [messages(g) for g in range(4)]

    def place(i, at, n):
        return i if isinstance(i, slice) else lax.rem(at + i + n, n)

    def send_weight(g, name, d, i):
        ring, zs, ys, rows, _, take = tables[g][name, d, i]
        ref = bufs[g].at[place(zs, z, NZ), place(ys, y, NY), rows, :]
        pltpu.make_async_remote_copy(
            src_ref=ref, dst_ref=ref, send_sem=send.at[g], recv_sem=recv.at[g, TAKES.index(take)],
            device_id=(ynb if ring == "y" else znb)[d], device_id_type=MESH,
        ).start()

    def wait_bytes(ref, sem):
        pltpu.make_async_copy(ref, ref, sem).wait()

    def take_weight(g, name, i):
        slabs, rows = 0, None
        for v in tables[g].values():
            if v[5] == (name, i):
                whole = extent(v[3])
                slabs += extent(v[1]) * extent(v[2]) * whole
        for nz, ny, size in ((1, 1, SLAB), (1, 2, SLAB), (1, 4, SLAB), (1, 8, SLAB), (2, 8, SLAB), (3, 8, SLAB)):
            if slabs % (nz * ny * 16) == 0 and slabs <= nz * ny * size:
                ref = bufs[g].at[0:nz, 0:ny, 0 : slabs // (nz * ny), :]
                wait_bytes(ref, recv.at[g, TAKES.index((name, i))])
                return
        raise ValueError(name)

    def norm_rows(i, c):
        r = pl.ds(pl.multiple_of(i * 16, 16), 16)
        v = tok[r, :].astype(F32)
        xn[r, :] = (v * lax.rsqrt(jnp.mean(v * v, axis=-1, keepdims=True) + EPS) * gain1[...]).astype(BF16)
        return c

    def norm():
        for c in fetches:
            c.wait()
        lax.fori_loop(0, SEQ // 16, norm_rows, 0)

    def build_mats(l, c):
        ti, si = iota((SEQ, 2 * SEQ), 0), lax.rem(iota((SEQ, 2 * SEQ), 1), SEQ)
        same = lax.shift_right_logical(ti, l) == lax.shift_right_logical(si, l)
        back = (ti - si) * (2 * (lax.shift_right_logical(ti, l) & 1) - 1)
        mats[2 * l] = jnp.where(same & (back >= 0), 1.0, 0.0).astype(BF16)
        mats[2 * l + 1] = jnp.where(same & (back > 0), 1.0, 0.0).astype(BF16)
        return c

    def build():
        lax.fori_loop(0, LEVELS, build_mats, 0)
        heads = jnp.where(lax.div(iota((HEADS, 128), 1), KW) == iota((HEADS, 128), 0), 1.0, 0.0)
        extra[...] = lax.dot_general(
            spike[...], heads, (((0,), (0,)), ((), ())), precision=lax.Precision.HIGHEST, preferred_element_type=F32
        )

    def project():
        acc[...] = jnp.zeros_like(acc)

        def body(w, c):
            cols = pl.ds(pl.multiple_of(w * 512, 512), 512)
            acc[...] += dot(xn[:, cols], g1[w].reshape(512, 640))
            return c

        lax.fori_loop(0, NZ, body, 0)

    lane_head = lax.div(iota((SEQ, 128), 1), KW)

    def by_head(x):
        return jnp.concatenate([jnp.where(lane_head == h, x, 0.0).astype(BF16) for h in range(HEADS)], axis=0)

    def prepare():
        gate = acc[:, 512:640] + bias[...]
        logs = (jnp.minimum(gate, 0.0) - jnp.log1p(jnp.exp(-jnp.abs(gate)))) / 16.0 + extra[...]
        hi = logs.astype(BF16)
        decay2[0:SEQ, :] = hi
        decay2[SEQ : 2 * SEQ, :] = (logs - hi.astype(F32)).astype(BF16)
        qf[...] = acc[:, 0:128].astype(BF16).astype(F32)
        kf[...] = acc[:, 128:256].astype(BF16).astype(F32)
        vals = acc[:, 256:512]
        lane_vhead = lax.div(iota((SEQ, 256), 1), VW)
        for h in range(HEADS):
            vbd[h * SEQ : (h + 1) * SEQ, :] = jnp.where(lane_vhead == h, vals, 0.0).astype(BF16)
        score[...] = 2.0 * dot_t(qf[...].astype(BF16), by_head(kf[...]))

    def level(l):
        left = (qf[...] * jnp.exp(dot(mats[2 * l], decay2[...]))).astype(BF16)
        right = by_head(kf[...] * jnp.exp(dot(mats[2 * l + 1], decay2[...])))
        differ = iota((SEQ, HEADS * SEQ), 0) ^ lax.rem(iota((SEQ, HEADS * SEQ), 1), SEQ)
        score[...] = jnp.where(differ >= 2 ** l, dot_t(left, right), score[...])

    def attend():
        mixed = dot(score[...].astype(BF16), vbd[...]) * (KW ** -0.5)
        sq = mixed * mixed
        sq_hi = sq.astype(BF16)
        sq_lo = (sq - sq_hi.astype(F32)).astype(BF16)
        ones = jnp.where(lax.div(iota((256, 256), 0), VW) == lax.div(iota((256, 256), 1), VW), 1.0, 0.0).astype(BF16)
        mean = (dot(sq_hi, ones) + dot(sq_lo, ones)) * (1.0 / VW)
        gains = jnp.concatenate([hgain[...]] * HEADS, axis=1)
        att[...] = (mixed * lax.rsqrt(mean + EPS) * gains).astype(BF16)

    def cols_of(c):
        return slice(c * D // CHUNKS, (c + 1) * D // CHUNKS)

    def copy_to(device, n, src, dst, sem):
        pltpu.make_async_remote_copy(
            src_ref=src, dst_ref=dst, send_sem=tsend.at[n], recv_sem=sem, device_id=device, device_id_type=MESH
        ).start()

    def slab_of(c):
        return lax.rem(z + SLAB_ORDER[c] + NZ, NZ)

    def project_out(n, c, left, weight, width):
        into, cols = parts[n], cols_of(c)
        rows = weight[c if n == 0 else slab_of(c)].reshape(D // NZ, width)
        into[:, :, :, cols] = dot_t(left[...], rows).astype(BF16).reshape(NTP // 2, 2, ROWS_OWN, D // NZ)
        copy_to(partner, n, into.at[:, 1 - core, :, cols], lands[n].at[:, :, cols], trecv.at[n, 0, c])

    def pair(n, c):
        cols = cols_of(c)
        both[n][:, :, cols] = (
            parts[n][:, core, :, cols].astype(F32) + lands[n][:, :, cols].astype(F32)
        ).astype(BF16)
        for k in (1, 2, 3):
            copy_to(peer(k), n, both[n].at[around(k), :, cols], gots[n].at[k - 1, :, cols], trecv.at[n, 1, c])

    def total(n, cols):
        s = parts[n][x, core, :, cols].astype(F32) + lands[n][x, :, cols].astype(F32)
        for k in range(3):
            s = s + gots[n][k, :, cols].astype(F32)
        return s

    own_rows = pl.ds(pl.multiple_of(t * ROWS_OWN, ROWS_OWN), ROWS_OWN)

    def residual(c):
        cols = cols_of(c)
        r = (tok[own_rows, cols].astype(F32) + total(0, cols)).astype(BF16).astype(F32)
        resid[:, cols] = r
        mine = n2.at[x, core, :, cols]
        mine[...] = (r * gain2[:, cols]).astype(BF16)
        pieces = [mine]
        if c == CHUNKS - 1:
            r = resid[...]
            factor = lax.rsqrt(jnp.mean(r * r, axis=-1, keepdims=True) + EPS)
            factors[x, core] = jnp.broadcast_to(factor, (ROWS_OWN, 128))
            pieces.append(factors.at[x, core])
        for piece in pieces:
            for k in (1, 2, 3):
                copy_to(peer(k), 0, piece, piece, trecv.at[0, 2, c])
            copy_to(partner, 0, piece, piece, trecv.at[0, 3, 0])

    def relay_normed(c):
        for k in (1, 2, 3):
            piece = n2.at[around(k), core, :, cols_of(c)]
            copy_to(partner, 0, piece, piece, trecv.at[0, 3, 0])
            if c == CHUNKS - 1:
                piece = factors.at[around(k), core]
                copy_to(partner, 0, piece, piece, trecv.at[0, 3, 0])

    def place_of(c):
        return pl.ds(pl.multiple_of(slab_of(c) * (D // NZ), D // NZ), D // NZ)

    def out_at(i, c):
        rows = pl.ds(pl.multiple_of((2 * i + core) * ROWS_OWN, ROWS_OWN), ROWS_OWN)
        return out.at[rows, place_of(c)]

    def put(i, c):
        piece = fin.at[i, :, cols_of(c)]
        copy_to(partner, 1, piece, out_at(i, c), trecv.at[1, 3, 0])
        pltpu.make_async_copy(piece, out_at(i, c), lsem.at[5]).start()

    def layer_out(c):
        cols, at = cols_of(c), place_of(c)
        fin[x, :, cols] = (resid[:, at] + total(1, cols)).astype(BF16)
        for k in (1, 2, 3):
            copy_to(peer(k), 1, fin.at[x, :, cols], fin.at[x, :, cols], trecv.at[1, 2, c])
        put(x, c)

    def relay_out(c):
        for k in (1, 2, 3):
            put(around(k), c)

    def end():
        wait_bytes(fin, lsem.at[5])

    def take_exchange(what):
        n, c = int(what[1]), int(what[2])
        kind = "dxsf".index(what[0])
        wide = D // CHUNKS + (256 if n == 0 and what[0] == "s" and c == CHUNKS - 1 else 0)
        ref = (lands if what[0] == "d" else gots)[n].at[:, :, 0:wide]
        if what[0] == "f":
            ref = parts[n].at[:, :, :, 0 : D // 2 + (128 if n == 0 else 0)]
        wait_bytes(ref, trecv.at[n, kind, c])

    def gate_up():
        acc2[...] = jnp.zeros_like(acc2)

        def body(w, c):
            cols = pl.ds(pl.multiple_of(w * 512, 512), 512)
            acc2[...] += dot(n2[:, :, :, cols].reshape(SEQ, 512), g3[w].reshape(512, 768))
            return c

        lax.fori_loop(0, NZ, body, 0)

    def hidden():
        factor = factors[...].reshape(SEQ, 128)[:, 0:1]
        gated = acc2[:, 0:384] * factor
        hid[...] = (gated / (1.0 + jnp.exp(-gated)) * (acc2[:, 384:768] * factor)).astype(BF16)

    work = dict(
        norm=norm, mats=build, project=project, prepare=prepare, attend=attend,
        gate_up=gate_up, hidden=hidden, end=end,
        levels0=lambda: [level(l) for l in range(4)], levels1=lambda: [level(l) for l in range(4, LEVELS)],
        **{f"pair{n}{c}": functools.partial(pair, n, c) for n in (0, 1) for c in range(CHUNKS)},
    )
    for c in range(CHUNKS):
        work[f"mix{c}"] = functools.partial(project_out, 0, c, att, g2, 256)
        work[f"down{c}"] = functools.partial(project_out, 1, c, hid, g4, 384)
        work[f"residual{c}"] = functools.partial(residual, c)
        work[f"relay0{c}"] = functools.partial(relay_normed, c)
        work[f"relay1{c}"] = functools.partial(relay_out, c)
        work[f"layer{c}"] = functools.partial(layer_out, c)
    waiting = set(range(4))
    for verb, what in link_plan(NEAR):
        with jax.named_scope(f"{verb}_{what}".replace(" ", "")):
            if verb == "work":
                work[what]()
            elif verb == "send":
                if what[0] in waiting:
                    waiting.discard(what[0])
                    own[what[0]].wait()
                send_weight(*what)
            elif isinstance(what, str):
                take_exchange(what)
            else:
                take_weight(*what)
    for g in range(4):
        wait_bytes(bufs[g].at[0:3], send.at[g])
        wait_bytes(bufs[g].at[3, 0:7], send.at[g])
    for n in (0, 1):
        wait_bytes(parts[n], tsend.at[n])
        wait_bytes(parts[n].at[0:3], tsend.at[n])
    wait_bytes(factors.at[0:3], tsend.at[0])
    wait_bytes(factors.at[3, 0], tsend.at[0])


def shards(
    tokens, attention_norm_gain, query_weight, key_weight, value_weight, decay_weight, decay_gate_bias,
    decay_spike_extra, head_output_gain, output_weight, channel_norm_gain, gate_weight, up_weight, down_weight,
):
    hbm = pl.BlockSpec(memory_space=pltpu.HBM)
    widths = [sum(p) for p in PARTS]
    return pl.pallas_call(
        layer_kernel,
        out_shape=jax.ShapeDtypeStruct((SEQ, D), BF16),
        in_specs=[hbm] * 14,
        out_specs=pl.BlockSpec(memory_space=pl.ANY),
        scratch_shapes=[
            pltpu.VMEM((SEQ, D), BF16),
            pltpu.VMEM((1, D), F32),
            pltpu.VMEM((1, 128), F32),
            pltpu.VMEM((HEADS, SEQ), F32),
            pltpu.VMEM((1, VW), F32),
            pltpu.VMEM((1, D), F32),
            pltpu.VMEM((SEQ, 128), F32),
            pltpu.VMEM((NTP // 2, ROWS_OWN, D), BF16),
            *(pltpu.VMEM((NZ, NY, SLAB, w), BF16) for w in widths),
            pltpu.VMEM((SEQ, D), BF16),
            pltpu.VMEM((SEQ, 640), F32),
            pltpu.VMEM((2 * LEVELS, SEQ, 2 * SEQ), BF16),
            pltpu.VMEM((SEQ, HEADS * SEQ), F32),
            pltpu.VMEM((SEQ, 256), BF16),
            pltpu.VMEM((NTP // 2, 2, ROWS_OWN, D), BF16),
            pltpu.VMEM((SEQ, 768), F32),
            pltpu.VMEM((SEQ, 384), BF16),
            pltpu.VMEM((ROWS_OWN, D), F32),
            pltpu.VMEM((2 * SEQ, 128), BF16),
            pltpu.VMEM((SEQ, 128), F32),
            pltpu.VMEM((SEQ, 128), F32),
            pltpu.VMEM((HEADS * SEQ, 256), BF16),
            *[pltpu.VMEM((NTP // 2, 2, ROWS_OWN, D), BF16)] * 2,
            *[pltpu.VMEM((NTP // 2, ROWS_OWN, D), BF16)] * 4,
            *[pltpu.VMEM((NTP // 2 - 1, ROWS_OWN, D), BF16)] * 2,
            pltpu.VMEM((NTP // 2, 2, ROWS_OWN, 128), F32),
            pltpu.SemaphoreType.DMA((12,)),
            pltpu.SemaphoreType.DMA((4,)),
            pltpu.SemaphoreType.DMA((4, len(TAKES))),
            pltpu.SemaphoreType.DMA((2,)),
            pltpu.SemaphoreType.DMA((2, 4, CHUNKS)),
        ],
        compiler_params=pltpu.CompilerParams(collective_id=0, has_side_effects=True),
    )(
        tokens,
        attention_norm_gain.reshape(1, D),
        decay_gate_bias.reshape(1, 128),
        decay_spike_extra.T,
        head_output_gain.reshape(1, VW),
        channel_norm_gain.reshape(1, D),
        query_weight, key_weight, value_weight, decay_weight, output_weight, gate_weight, up_weight, down_weight,
    )


def solution(mesh):
    rows, w = P(("rep", "fs"), None), P("fs", "tp")
    in_specs = (rows, P(), w, w, w, w, P("tp"), P(("rep", "fs"), "tp"), P(), w, P(), w, w, w)
    return jax.shard_map(shards, mesh=mesh, in_specs=in_specs, out_specs=rows, check_vma=False)
```
